256 devices in a mesh: kv: 32 (over z, y), tp: 8 (over x, core).
Axes of the slice: x: 4, y: 4, z: 8, core: 2. Of those that a mesh axis runs over, the one named last changes fastest.
Arguments:
- residual: bfloat16 [1024, 2048], P('kv', 'tp'), may hold values from -12 to 12
- first_gain: bfloat16 [2048], P('tp'), may hold values from 0.099609375 to 1.8984375
- first_gate: bfloat16 [2048, 5632], P('tp', 'kv'), may hold values from -0.125 to 0.125
- first_lift: bfloat16 [2048, 5632], P('tp', 'kv'), may hold values from -0.125 to 0.125
- first_down: bfloat16 [5632, 2048], P('kv', 'tp'), may hold values from -0.078125 to 0.078125
- mixer_gain: bfloat16 [2048], replicated, may hold values from 0.099609375 to 1.8984375
- proj_gate: bfloat16 [2048, 2048], P(None, 'tp'), may hold values from -0.125 to 0.125
- proj_input: bfloat16 [2048, 2048], P(None, 'tp'), may hold values from -0.125 to 0.125
- proj_write: bfloat16 [2048, 1024], P(None, 'tp'), may hold values from -0.125 to 0.125
- proj_read: bfloat16 [2048, 1024], P(None, 'tp'), may hold values from -0.125 to 0.125
- proj_step: bfloat16 [2048, 32], P(None, 'tp'), may hold values from -0.125 to 0.125
- step_bias: float32 [32], P('tp'), may hold values from -5 to -2
- rate_log: float32 [32], P('tp'), may hold values from -0.7 to 2.1
- skip_gain: float32 [32], P('tp'), may hold values from 0.5 to 2
- taps_input: bfloat16 [4, 2048], P(None, 'tp'), may hold values from -3 to 3
- taps_write: bfloat16 [4, 1024], P(None, 'tp'), may hold values from -3 to 3
- taps_read: bfloat16 [4, 1024], P(None, 'tp'), may hold values from -3 to 3
- buffer_input: bfloat16 [1024, 3, 2048], P('kv', None, 'tp'), may hold values from -6 to 6
- buffer_write: bfloat16 [1024, 3, 1024], P('kv', None, 'tp'), may hold values from -6 to 6
- buffer_read: bfloat16 [1024, 3, 1024], P('kv', None, 'tp'), may hold values from -6 to 6
- scan_state: float32 [1024, 32, 64, 128], P('kv', 'tp'), may hold values from -1.5 to 1.5
- group_gain: bfloat16 [2048], P('tp'), may hold values from 0.099609375 to 1.8984375
- proj_output: bfloat16 [2048, 2048], P('tp'), may hold values from -0.125 to 0.125
- second_gain: bfloat16 [2048], P('tp'), may hold values from 0.099609375 to 1.8984375
- second_gate: bfloat16 [2048, 5632], P('tp', 'kv'), may hold values from -0.125 to 0.125
- second_lift: bfloat16 [2048, 5632], P('tp', 'kv'), may hold values from -0.125 to 0.125
- second_down: bfloat16 [5632, 2048], P('kv', 'tp'), may hold values from -0.078125 to 0.078125
Outputs:
- residual_out: bfloat16 [1024, 2048], P('kv', 'tp')
- state_out: float32 [1024, 32, 64, 128], P('kv', 'tp')
The draws below stay inside these ranges and needn't reach their ends.
All inputs are finite; a program needn't handle non-finite values.
Results may differ from the reference program's by a relative error of at most 0.023.
Values may be sent and summed in bfloat16 or wider, within the bound.
A program may use at most 64 MiB of HBM per device.

```python
import jax
import jax.numpy as jnp
from jax import lax

D = 2048
FF = 5632
HEADS = 32
HEAD_DIM = 64
STATE = 128
NGROUPS = 8
CONV = 4
D_SSD = 2048
BATCH = 1024
N_TP = 8


def draw_residual(key, part):
    first_key = jax.random.fold_in(key, 0)
    columns = jnp.arange(D, dtype=jnp.float32)
    column_ramp = 0.5 * jnp.power(4.0, columns / (D - 1))
    entries = jax.random.normal(first_key, (BATCH, D), jnp.float32)
    return jnp.clip(entries * column_ramp[None, :], -12.0, 12.0).astype(jnp.bfloat16)


def steps_of(own_key, extent, cuts, least, largest):
    level, own = 1.0, jax.random.fold_in(own_key, 6)
    for position, shards_of in cuts:
        heights = jnp.exp(jax.random.uniform(jax.random.fold_in(own, position), (shards_of,), jnp.float32, least / len(cuts), largest / len(cuts)))
        level = level * jnp.repeat(heights, extent[position] // shards_of).reshape([-1 if axis == position else 1 for axis in range(len(extent))])
    return level


def gaussian(key, dims, width, most, shards=(), held_as=jnp.bfloat16):
    level = steps_of(key, dims, shards, -0.22, 0.18) if shards else 1.0
    values = jax.random.normal(key, dims, jnp.float32) * width * level
    return jnp.minimum(jnp.maximum(values, -most), most).astype(held_as)


def setup_inputs(seed: int = 0) -> dict:
    seeds = jax.random.split(jax.random.key(seed), 28)
    return {
        "residual": draw_residual(jax.random.fold_in(seeds[27], 71), 0),
        "first_gain": jnp.clip(1.0 + 0.18 * jax.random.normal(seeds[1], (D,), jnp.float32), 0.099609375, 1.8984375).astype(jnp.bfloat16),
        "first_gate": gaussian(seeds[2], (D, FF), D ** -0.5, 0.125, ((0, 8), (1, 32))),
        "first_lift": gaussian(seeds[3], (D, FF), D ** -0.5, 0.125, ((0, 8), (1, 32))),
        "first_down": gaussian(seeds[4], (FF, D), FF ** -0.5, 0.078125, ((0, 32), (1, 8))),
        "mixer_gain": jnp.clip(1.0 + 0.18 * jax.random.normal(seeds[5], (D,), jnp.float32), 0.099609375, 1.8984375).astype(jnp.bfloat16),
        "proj_gate": gaussian(seeds[6], (D, D_SSD), D ** -0.5, 0.125, ((1, 8),)),
        "proj_input": gaussian(seeds[7], (D, D_SSD), D ** -0.5, 0.125, ((1, 8),)),
        "proj_write": gaussian(seeds[8], (D, NGROUPS * STATE), D ** -0.5, 0.125, ((1, 8),)),
        "proj_read": gaussian(seeds[9], (D, NGROUPS * STATE), D ** -0.5, 0.125, ((1, 8),)),
        "proj_step": gaussian(seeds[10], (D, HEADS), D ** -0.5, 0.125, ((1, 8),)),
        "step_bias": jnp.clip(-5.0 + 3.0 * jax.random.uniform(seeds[11], (HEADS,), jnp.float32) ** steps_of(seeds[11], (HEADS,), ((0, 8),), -0.2, 0.2), -5.0, -2.0),
        "rate_log": jnp.clip(-0.7 + 2.8 * jax.random.uniform(seeds[12], (HEADS,), jnp.float32) ** steps_of(seeds[12], (HEADS,), ((0, 8),), -0.2, 0.2), -0.7, 2.1),
        "skip_gain": jnp.clip(0.5 + 1.5 * jax.random.uniform(seeds[13], (HEADS,), jnp.float32) ** steps_of(seeds[13], (HEADS,), ((0, 8),), -0.2, 0.2), 0.5, 2.0),
        "taps_input": gaussian(seeds[14], (CONV, D_SSD), CONV ** -0.5, 3.0, ((1, 8),)),
        "taps_write": gaussian(seeds[15], (CONV, NGROUPS * STATE), CONV ** -0.5, 3.0, ((1, 8),)),
        "taps_read": gaussian(seeds[16], (CONV, NGROUPS * STATE), CONV ** -0.5, 3.0, ((1, 8),)),
        "buffer_input": gaussian(seeds[17], (BATCH, CONV - 1, D_SSD), 1.0, 6.0, ((0, 32), (2, 8))),
        "buffer_write": gaussian(seeds[18], (BATCH, CONV - 1, NGROUPS * STATE), 1.0, 6.0, ((0, 32), (2, 8))),
        "buffer_read": gaussian(seeds[19], (BATCH, CONV - 1, NGROUPS * STATE), 1.0, 6.0, ((0, 32), (2, 8))),
        "scan_state": gaussian(seeds[20], (BATCH, HEADS, HEAD_DIM, STATE), 0.1, 1.5, ((0, 32), (1, 8)), jnp.float32),
        "group_gain": jnp.clip(1.0 + 0.18 * jax.random.normal(seeds[21], (D_SSD,), jnp.float32), 0.099609375, 1.8984375).astype(jnp.bfloat16),
        "proj_output": gaussian(seeds[22], (D_SSD, D), D_SSD ** -0.5, 0.125, ((0, 8),)),
        "second_gain": jnp.clip(1.0 + 0.18 * jax.random.normal(seeds[23], (D,), jnp.float32), 0.099609375, 1.8984375).astype(jnp.bfloat16),
        "second_gate": gaussian(seeds[24], (D, FF), D ** -0.5, 0.125, ((0, 8), (1, 32))),
        "second_lift": gaussian(seeds[25], (D, FF), D ** -0.5, 0.125, ((0, 8), (1, 32))),
        "second_down": gaussian(seeds[26], (FF, D), FF ** -0.5, 0.078125, ((0, 32), (1, 8))),
    }


norm_eps = 1e-06

def inverse_rms(values):
    return lax.rsqrt(lax.optimization_barrier(jnp.mean(values * values, axis=-1, keepdims=True)) + norm_eps)

def block_sum(activ, weight, pieces):
    seq_rows = activ.shape[0]
    inner = activ.shape[1] // pieces
    widened = lax.optimization_barrier(activ).astype(jnp.float32).reshape(seq_rows, pieces, inner)
    weight_f = weight.astype(jnp.float32).reshape(pieces, inner, weight.shape[1])
    partial_value = jnp.einsum('btk,tkf->tbf', widened, weight_f)
    rounded = lax.optimization_barrier(partial_value.astype(jnp.bfloat16)).astype(jnp.float32)
    return lax.optimization_barrier(jnp.sum(rounded, axis=0))

def half_step(residual, gain, gate_weight, lift_weight, down_weight):
    widened = residual.astype(jnp.float32)
    normed = (widened * inverse_rms(widened) * gain.astype(jnp.float32)).astype(jnp.bfloat16)
    gate_sum = block_sum(normed, gate_weight, N_TP)
    up_sum = block_sum(normed, lift_weight, N_TP)
    hidden = (jax.nn.silu(gate_sum) * up_sum).astype(jnp.bfloat16)
    branch = jnp.dot(hidden, down_weight, preferred_element_type=jnp.float32)
    return (widened + 0.5 * branch).astype(jnp.bfloat16)

def short_conv(tap_weights, buffer, newest):
    taps_f = tap_weights.astype(jnp.float32)
    summed = lax.optimization_barrier(jnp.sum(buffer.astype(jnp.float32) * taps_f[None, :-1, :], axis=1))
    summed = summed + newest.astype(jnp.float32) * taps_f[-1][None, :]
    return jax.nn.silu(summed)

def state_mixer(residual, mixer_gain, proj_gate, proj_input, proj_write, proj_read, proj_step, step_bias, rate_log, skip_gain, taps_input, taps_write, taps_read, buffer_input, buffer_write, buffer_read, scan_state, group_gain, proj_output):
    seq_rows = residual.shape[0]
    widened = residual.astype(jnp.float32)
    normed = (widened * inverse_rms(widened) * mixer_gain.astype(jnp.float32)).astype(jnp.bfloat16)

    def project(weight):
        return jnp.dot(normed, weight, preferred_element_type=jnp.float32).astype(jnp.bfloat16)
    gate_z = project(proj_gate)
    input_new = project(proj_input)
    write_new = project(proj_write)
    read_new = project(proj_read)
    step_raw = project(proj_step)
    input_conv = short_conv(taps_input, buffer_input, input_new)
    write_conv = short_conv(taps_write, buffer_write, write_new)
    read_conv = short_conv(taps_read, buffer_read, read_new)
    head_count = proj_step.shape[1]
    group_count = proj_write.shape[1] // STATE
    per_group = head_count // group_count
    step = jax.nn.softplus(step_raw.astype(jnp.float32) + step_bias[None, :])
    retain = jnp.exp(-step * jnp.exp(rate_log)[None, :])
    input_heads = input_conv.reshape(seq_rows, group_count, per_group, HEAD_DIM)
    write_groups = write_conv.reshape(seq_rows, group_count, STATE)
    read_groups = read_conv.reshape(seq_rows, group_count, STATE)
    old_state = scan_state.reshape(seq_rows, group_count, per_group, HEAD_DIM, STATE)
    retain_g = retain.reshape(seq_rows, group_count, per_group)
    step_g = step.reshape(seq_rows, group_count, per_group)
    updated = retain_g[..., None, None] * old_state + (step_g[..., None] * input_heads)[..., None] * write_groups[:, :, None, None, :]
    head_out = jnp.einsum('bgrpn,bgn->bgrp', updated, read_groups, precision=lax.Precision.HIGHEST)
    head_out = head_out + skip_gain.reshape(group_count, per_group)[None, :, :, None] * input_heads
    head_short = lax.optimization_barrier(head_out.astype(jnp.bfloat16))
    gated = head_short.astype(jnp.float32).reshape(seq_rows, group_count, per_group * HEAD_DIM)
    gated = gated * jax.nn.silu(gate_z.astype(jnp.float32).reshape(seq_rows, group_count, per_group * HEAD_DIM))
    gated = gated * inverse_rms(gated) * group_gain.astype(jnp.float32).reshape(group_count, per_group * HEAD_DIM)[None]
    gated = gated.reshape(seq_rows, head_count * HEAD_DIM).astype(jnp.bfloat16)
    mixed = block_sum(gated, proj_output, N_TP)
    return ((widened + mixed).astype(jnp.bfloat16), updated.reshape(seq_rows, head_count, HEAD_DIM, STATE))

def reference(residual, first_gain, first_gate, first_lift, first_down, mixer_gain, proj_gate, proj_input, proj_write, proj_read, proj_step, step_bias, rate_log, skip_gain, taps_input, taps_write, taps_read, buffer_input, buffer_write, buffer_read, scan_state, group_gain, proj_output, second_gain, second_gate, second_lift, second_down):
    first = half_step(residual, first_gain, first_gate, first_lift, first_down)
    mixed, state_out = state_mixer(first, mixer_gain, proj_gate, proj_input, proj_write, proj_read, proj_step, step_bias, rate_log, skip_gain, taps_input, taps_write, taps_read, buffer_input, buffer_write, buffer_read, scan_state, group_gain, proj_output)
    residual_out = half_step(mixed, second_gain, second_gate, second_lift, second_down)
    return (residual_out, state_out)
```

```python
import jax
import jax.numpy as jnp
from jax import lax
from jax.experimental import pallas as pl
from jax.experimental.pallas import tpu as pltpu
from jax.sharding import PartitionSpec as P

D = 2048
HEAD_DIM = 64
STATE = 128
EPS = 1e-06

NZ, NY, NT = 8, 4, 8
NKV = NZ * NY
RPT = 4
QW = 512
SEQ = 32
GROUP = 256
Z_ORDER_NEAR = (1, 7, 2, 6, 3, 5, 4)
Z_ORDER_FAR = (4, 3, 5, 2, 6, 1, 7, 0)
MESH = pl.DeviceIdType.MESH
F32, BF16 = jnp.float32, jnp.bfloat16


def dot(a, b):
    return jnp.dot(a, b, preferred_element_type=F32)


def iota2(shape, dim):
    return lax.broadcasted_iota(jnp.int32, shape, dim)


def gather_rows(n):
    shape = (16 * n, 16 * n)
    row, col = iota2(shape, 0), iota2(shape, 1)
    q, rest = row // (4 * n), row % (4 * n)
    return (col == (rest // 4) * 16 + q * 4 + rest % 4).astype(BF16)


def scatter_rows(n):
    shape = (16 * n, 16 * n)
    row, col = iota2(shape, 0), iota2(shape, 1)
    q, rest = col // (4 * n), col % (4 * n)
    return (row == (rest // 4) * 16 + q * 4 + rest % 4).astype(BF16)


def piece_factor(piece):
    partial = jnp.sum(piece * piece, axis=1, keepdims=True)
    same = (iota2((16, 16), 0) % 4 == iota2((16, 16), 1) % 4).astype(F32)
    total = jnp.dot(
        same,
        jnp.broadcast_to(partial, (16, 128)),
        preferred_element_type=F32,
        precision=lax.Precision.HIGHEST,
    )
    return lax.rsqrt(total[:, :1] / D + EPS)


def kernel(
    msg_ref, mgain_ref, par_ref, conv_ref,
    fg_ref, fl_ref, fd_ref, sg_ref, sl_ref, sd_ref,
    pg_ref, pi_ref, pw_ref, pr_ref, ps_ref, po_ref, scan_ref,
    out_ref, retain_ref, u_ref, bc_ref,
    recv_r, wg1, wl1, wd1, wg2, wl2, wd2,
    ag1, ag2, perm, permt, hid, psend, ry1, zs1, rz1, ry2, zs2, rz2,
    send_f, recv_f, recv_o, send_o, send_q, recv_q,
    pgv, piv, pwv, prv, psv, pov, scan_f, scan_b, xrow, gsplit,
    loc_sem, s_r, r_r, s_w, r_w, s_ag, r_ag, s_y, r_y, s_z, r_z, s_f, r_f, s_o, r_o, s_q, r_q,
):
    kv = lax.axis_index("kv")
    t = lax.axis_index("tp")
    z, y = kv // NY, kv % NY
    core = t % 2

    def zpeer(d):
        return lax.rem(z + d, NZ)

    def ypeer(d):
        return lax.rem(y + d, NY)

    def tpeer(d):
        return lax.rem(t + d, NT)

    def rcopy(src, dst, ssem, rsem, dev):
        return pltpu.make_async_remote_copy(
            src_ref=src, dst_ref=dst, send_sem=ssem, recv_sem=rsem, device_id=dev, device_id_type=MESH
        )

    locals_ = []

    def local(src, dst, k):
        copy = pltpu.make_async_copy(src, dst, loc_sem.at[k])
        copy.start()
        return copy

    l_msg = local(msg_ref.at[t], recv_r.at[t], 0)
    l_w1 = [local(fg_ref, wg1.at[t], 1), local(fl_ref, wl1.at[t], 2), local(fd_ref, wd1.at[t], 3)]

    barrier = pltpu.get_barrier_semaphore()
    peers = [(zpeer(d) * NY + y, t) for d in range(1, NZ)]
    peers += [(z * NY + ypeer(d), t) for d in range(1, NY)]
    peers += [(kv, tpeer(d)) for d in range(1, NT)]
    for dev in peers:
        pl.semaphore_signal(barrier, inc=1, device_id=dev, device_id_type=MESH)

    perm[...] = gather_rows(NKV)
    permt[...] = scatter_rows(NKV)
    pl.semaphore_wait(barrier, len(peers))

    sends_r = []
    for d in range(1, NT):
        tt = tpeer(d)
        c = rcopy(msg_ref.at[tt], recv_r.at[t], s_r.at[d], r_r.at[d], (kv, tt))
        c.start()
        sends_r.append(c)

    def start_weights(k, src, dst):
        copies = []
        for j in range(1, 4):
            tt = lax.rem(t + 2 * j, NT)
            c = rcopy(src, dst.at[t], s_w.at[k, j], r_w.at[k, j], (kv, tt))
            c.start()
            copies.append(c)
        c = rcopy(src, dst.at[t], s_w.at[k, 0], r_w.at[k, 0], (kv, t + 1 - 2 * core))
        c.start()
        copies.append(c)
        return copies

    def forward_weights(k, dst):
        copies = []
        for j in range(1, 4):
            ss = lax.rem(t - 2 * j + NT, NT)
            rcopy(dst.at[ss], dst.at[ss], s_w.at[k, j], r_w.at[k, j], (kv, ss)).wait_recv()
            c = rcopy(dst.at[ss], dst.at[ss], s_w.at[k, 3 + j], r_w.at[k, 3 + j], (kv, t + 1 - 2 * core))
            c.start()
            copies.append(c)
        return copies

    def finish_weights(k, dst, copies):
        partner = t + 1 - 2 * core
        rcopy(dst.at[partner], dst.at[partner], s_w.at[k, 0], r_w.at[k, 0], (kv, partner)).wait_recv()
        for j in range(1, 4):
            ss = lax.rem(partner - 2 * j + NT, NT)
            rcopy(dst.at[ss], dst.at[ss], s_w.at[k, 3 + j], r_w.at[k, 3 + j], (kv, partner)).wait_recv()
        for c in copies:
            c.wait_send()

    w1 = [start_weights(0, fg_ref, wg1), start_weights(1, fl_ref, wl1), start_weights(2, fd_ref, wd1)]

    l_mix = [
        local(pg_ref, pgv, 4), local(pi_ref, piv, 5), local(pw_ref, pwv, 6), local(pr_ref, prv, 7),
        local(ps_ref, psv, 8), local(po_ref, pov, 9), local(scan_ref, scan_f, 10),
    ]
    l_w2 = [local(sg_ref, wg2.at[t], 11), local(sl_ref, wl2.at[t], 12), local(sd_ref, wd2.at[t], 13)]

    l_msg.wait()
    for d in range(1, NT):
        src = lax.rem(t - d + NT, NT)
        rcopy(recv_r.at[src], recv_r.at[src], s_r.at[d], r_r.at[d], (kv, src)).wait_recv()

    row, col = iota2((48, 64), 0), iota2((48, 64), 1)
    pick = (col == ((row % 16) // 4) * 16 + (row // 16) * 4 + row % 4).astype(BF16)
    halves = []
    for h in range(2):
        block = jnp.concatenate([recv_r[2 * q + h] for q in range(4)], axis=0)
        halves.append(dot(pick, block))
    both = jnp.concatenate(halves, axis=1)
    res1 = both[0:16]
    gsplit[...] = both[16:48]

    def start_gather(ag, f):
        me = kv
        copies = []
        for d in (4, 3, 5, 2, 6, 1, 7):
            c = rcopy(ag.at[me], ag.at[me], s_ag.at[f, 0, d], r_ag.at[f, 0, d], (zpeer(d) * NY + y, t))
            c.start()
            copies.append(c)
        for e in (2, 1, 3):
            c = rcopy(ag.at[me], ag.at[me], s_ag.at[f, e, 0], r_ag.at[f, e, 0], (z * NY + ypeer(e), t))
            c.start()
            copies.append(c)
        return copies

    def forward_gather(ag, f, copies):
        for d in Z_ORDER_NEAR:
            slot = lax.rem(z - d + NZ, NZ) * NY + y
            rcopy(ag.at[slot], ag.at[slot], s_ag.at[f, 0, d], r_ag.at[f, 0, d], (slot, t)).wait_recv()
            for e in (2, 1, 3):
                c = rcopy(ag.at[slot], ag.at[slot], s_ag.at[f, e, d], r_ag.at[f, e, d], (z * NY + ypeer(e), t))
                c.start()
                copies.append(c)

    def finish_gather(ag, f, copies):
        for d in (0,) + Z_ORDER_NEAR:
            for e in (1, 3, 2):
                slot = lax.rem(z - d + NZ, NZ) * NY + lax.rem(y - e + NY, NY)
                src = z * NY + lax.rem(y - e + NY, NY)
                rcopy(ag.at[slot], ag.at[slot], s_ag.at[f, e, d], r_ag.at[f, e, d], (src, t)).wait_recv()
        for c in copies:
            c.wait_send()

    def feed_forward(ag, wg, wl, wd):
        flat = ag[...].reshape(16 * NKV, QW)
        lhs = dot(perm[...], flat).astype(BF16)
        gate, lift = None, None
        for s in range(NT):
            q, h = s // 2, s % 2
            part = lhs[128 * q : 128 * q + 128, 256 * h : 256 * h + 256]
            g, u = dot(part, wg[s]), dot(part, wl[s])
            gate = g if gate is None else gate + g
            lift = u if lift is None else lift + u
        hidden = (gate * jax.nn.sigmoid(gate) * lift).astype(BF16)
        for s in range(NT):
            q, h = s // 2, s % 2
            hid[128 * q : 128 * q + 128, 256 * h : 256 * h + 256] = dot(hidden, wd[s]).astype(BF16)
        psend[...] = dot(permt[...], hid[...]).astype(BF16).reshape(NKV, 16, QW)

    def reduce_start(ry, f):
        copies = []
        for d in Z_ORDER_FAR:
            zz = zpeer(d)
            for e in (2, 1, 3):
                yy = ypeer(e)
                c = rcopy(psend.at[zz * NY + yy], ry.at[e, d], s_y.at[f, e, d], r_y.at[f, e, d], (z * NY + yy, t))
                c.start()
                copies.append(c)
        return copies

    def reduce_finish(ry, zs, rz, f, copies):
        own = None
        for d in Z_ORDER_FAR:
            zz = zpeer(d)
            total = psend[zz * NY + y].astype(F32)
            for e in (1, 3, 2):
                src = z * NY + lax.rem(y - e + NY, NY)
                rcopy(psend.at[0], ry.at[e, d], s_y.at[f, e, d], r_y.at[f, e, d], (src, t)).wait_recv()
                total = total + ry[e, d].astype(F32)
            if d == 0:
                own = total
            else:
                zs[d] = total.astype(BF16)
                c = rcopy(zs.at[d], rz.at[d], s_z.at[f, d], r_z.at[f, d], (zz * NY + y, t))
                c.start()
                copies.append(c)
        for d in range(1, NZ):
            src = lax.rem(z - d + NZ, NZ) * NY + y
            rcopy(zs.at[d], rz.at[d], s_z.at[f, d], r_z.at[f, d], (src, t)).wait_recv()
            own = own + rz[d].astype(F32)
        for c in copies:
            c.wait_send()
        return own

    ag1[kv] = (res1 * piece_factor(res1) * gsplit[0:16]).astype(BF16)
    a_copies = start_gather(ag1, 0)
    forward_gather(ag1, 0, a_copies)
    for k, dst in enumerate((wg1, wl1, wd1)):
        w1[k] += forward_weights(k, dst)
    finish_gather(ag1, 0, a_copies)
    for copy in l_w1:
        copy.wait()
    for k, dst in enumerate((wg1, wl1, wd1)):
        finish_weights(k, dst, w1[k])
    feed_forward(ag1, wg1, wl1, wd1)
    y_copies = reduce_start(ry1, 0)
    w2 = [start_weights(3, sg_ref, wg2), start_weights(4, sl_ref, wl2)]
    for copy in l_mix:
        copy.wait()
    scan_b[...] = scan_f[...].astype(BF16)
    branch = reduce_finish(ry1, zs1, rz1, 0, y_copies)
    first = (res1 + 0.5 * branch).astype(BF16).astype(F32)

    send_f[...] = (first * piece_factor(first) * mgain_ref[...]).astype(BF16)
    f_copies = []
    for d in range(1, NT):
        c = rcopy(send_f, recv_f.at[d], s_f.at[d], r_f.at[d], (kv, tpeer(d)))
        c.start()
        f_copies.append(c)
    recv_f[0] = send_f[...]
    row, col = iota2((128, 128), 0), iota2((128, 128), 1)
    q_, i_, r_ = row // 32, (row % 32) // 4, row % 4
    slot_ = lax.rem(t - i_ + NT, NT)
    perm8 = (col == slot_ * 16 + q_ * 4 + r_).astype(BF16)
    for d in range(1, NT):
        src = lax.rem(t - d + NT, NT)
        rcopy(send_f, recv_f.at[d], s_f.at[d], r_f.at[d], (kv, src)).wait_recv()
    rows = dot(perm8, recv_f[...].reshape(128, QW)).astype(BF16)
    for q in range(4):
        xrow[:, QW * q : QW * q + QW] = rows[32 * q : 32 * q + 32]
    mixed_in = xrow[...]

    def project(w):
        return dot(mixed_in, w[...]).astype(BF16).astype(F32)

    gate_z, input_new = project(pgv), project(piv)
    write_new, read_new, step_raw4 = project(pwv), project(prv), project(psv)

    def silu(v):
        return v * jax.nn.sigmoid(v)

    xc = silu(conv_ref[:, 0:256] + input_new * par_ref[4:5, :])
    bc = silu(conv_ref[:, 256:384] + write_new * par_ref[5:6, 0:128])
    rc = silu(conv_ref[:, 384:512] + read_new * par_ref[5:6, 128:256])
    lane_head = iota2((SEQ, GROUP), 1) // HEAD_DIM
    step_raw = jnp.zeros((SEQ, GROUP), F32)
    for h in range(4):
        step_raw = jnp.where(lane_head == h, step_raw4[:, h : h + 1], step_raw)
    pre = step_raw + par_ref[0:1, :]
    step = jnp.maximum(pre, 0.0) + jnp.log1p(jnp.exp(-jnp.abs(pre)))
    retain = jnp.exp(-step * jnp.exp(par_ref[1:2, :]))
    u = step * xc
    retain_ref[...] = retain
    u_ref[...] = u
    bc_ref[...] = bc
    rcb = rc.astype(BF16)
    sub = iota2((8, GROUP), 0)
    reads = []
    for g in range(4):
        acc = jnp.zeros((8, GROUP), F32)
        for j in range(8):
            b = 8 * g + j
            got = lax.dot_general(
                rcb[8 * g : 8 * g + 8], scan_b[b], (((1,), (1,)), ((), ())), preferred_element_type=F32
            )
            acc = jnp.where(sub == j, got, acc)
        reads.append(acc)
    read = jnp.concatenate(reads, axis=0)
    head = retain * read + u * jnp.sum(bc * rc, axis=1, keepdims=True) + par_ref[2:3, :] * xc
    gated = head.astype(BF16).astype(F32) * silu(gate_z)
    gated = gated * lax.rsqrt(jnp.mean(gated * gated, axis=1, keepdims=True) + EPS) * par_ref[3:4, :]
    part = dot(gated.astype(BF16), pov[...]).astype(BF16)
    stacked = jnp.concatenate([part[:, QW * q : QW * q + QW] for q in range(4)], axis=0)
    send_o[...] = dot(scatter_rows(NT), stacked).astype(BF16).reshape(NT, 16, QW)
    o_copies = []
    for d in range(1, NT):
        tt = tpeer(d)
        c = rcopy(send_o.at[tt], recv_o.at[d], s_o.at[d], r_o.at[d], (kv, tt))
        c.start()
        o_copies.append(c)
    for copy in l_w2:
        copy.wait()
    w2.append(start_weights(5, sd_ref, wd2))
    mixed = first + send_o[t].astype(F32)
    for d in range(1, NT):
        src = lax.rem(t - d + NT, NT)
        rcopy(send_f, recv_o.at[d], s_o.at[d], r_o.at[d], (kv, src)).wait_recv()
        mixed = mixed + recv_o[d].astype(F32)
    res2 = mixed.astype(BF16).astype(F32)

    ag2[kv] = (res2 * piece_factor(res2) * gsplit[16:32]).astype(BF16)
    a_copies = start_gather(ag2, 1)
    w2[0] += forward_weights(3, wg2)
    w2[1] += forward_weights(4, wl2)
    forward_gather(ag2, 1, a_copies)
    w2[2] += forward_weights(5, wd2)
    finish_gather(ag2, 1, a_copies)
    for k, dst in enumerate((wg2, wl2, wd2)):
        finish_weights(3 + k, dst, w2[k])
    feed_forward(ag2, wg2, wl2, wd2)
    y_copies = reduce_start(ry2, 1)
    branch = reduce_finish(ry2, zs2, rz2, 1, y_copies)
    final = (res2 + 0.5 * branch).astype(BF16)

    row, col = iota2((64, 16), 0), iota2((64, 16), 1)
    spread = ((col == (row // 16) * 4 + row % 16) & (row % 16 < 4)).astype(BF16)
    for h in range(2):
        block = dot(spread, final[:, 256 * h : 256 * h + 256]).astype(BF16).reshape(4, 16, 256)
        for q in range(4):
            send_q[2 * q + h] = block[q]
    q_copies = []
    for d in range(1, NT):
        tt = tpeer(d)
        c = rcopy(send_q.at[tt], recv_q.at[d], s_q.at[d], r_q.at[d], (kv, tt))
        c.start()
        q_copies.append(c)
    recv_q[0] = send_q[t]
    for d in range(1, NT):
        src = lax.rem(t - d + NT, NT)
        rcopy(send_q.at[0], recv_q.at[d], s_q.at[d], r_q.at[d], (kv, src)).wait_recv()
    row, col = iota2((32, 128), 0), iota2((32, 128), 1)
    pick32 = (col == lax.rem(t - row // 4 + NT, NT) * 16 + row % 4).astype(BF16)
    out_ref[...] = dot(pick32, recv_q[...].reshape(128, 256)).astype(BF16)

    for c in sends_r + f_copies + o_copies + q_copies:
        c.wait_send()


def per_device(
    residual, first_gain, first_gate, first_lift, first_down, mixer_gain,
    proj_gate, proj_input, proj_write, proj_read, proj_step,
    step_bias, rate_log, skip_gain, taps_input, taps_write, taps_read,
    buffer_input, buffer_write, buffer_read, scan_state, group_gain, proj_output,
    second_gain, second_gate, second_lift, second_down,
):
    msg = jnp.concatenate(
        [
            residual.reshape(NT, RPT, GROUP),
            jnp.broadcast_to(first_gain[None, None, :], (NT, RPT, GROUP)),
            jnp.broadcast_to(second_gain[None, None, :], (NT, RPT, GROUP)),
            jnp.zeros((NT, RPT, GROUP), BF16),
        ],
        axis=1,
    )
    mgain = jnp.repeat(mixer_gain.astype(F32).reshape(4, QW), RPT, axis=0)
    taps = jnp.concatenate([taps_input, taps_write, taps_read], axis=1).astype(F32)
    conv = jnp.concatenate(
        [
            jnp.sum(buf.astype(F32) * tap[None, :3, :].astype(F32), axis=1)
            for buf, tap in ((buffer_input, taps_input), (buffer_write, taps_write), (buffer_read, taps_read))
        ],
        axis=1,
    )
    par = jnp.stack(
        [
            jnp.repeat(step_bias, HEAD_DIM), jnp.repeat(rate_log, HEAD_DIM), jnp.repeat(skip_gain, HEAD_DIM),
            group_gain.astype(F32), taps[3, :256], taps[3, 256:], taps[3, :256], taps[3, 256:],
        ]
    )
    scan = scan_state.reshape(SEQ, GROUP, STATE)
    vm = pl.BlockSpec(memory_space=pltpu.VMEM)
    anym = pl.BlockSpec(memory_space=pl.ANY)
    hid_cols = first_gate.shape[1]
    dma = pltpu.SemaphoreType.DMA
    out, retain, u, bc = pl.pallas_call(
        kernel,
        out_shape=(
            jax.ShapeDtypeStruct((SEQ, GROUP), BF16),
            jax.ShapeDtypeStruct((SEQ, GROUP), F32),
            jax.ShapeDtypeStruct((SEQ, GROUP), F32),
            jax.ShapeDtypeStruct((SEQ, STATE), F32),
        ),
        in_specs=[vm] * 4 + [anym] * 13,
        out_specs=(vm,) * 4,
        scratch_shapes=[
            pltpu.VMEM((NT, 16, GROUP), BF16),
            *[pltpu.VMEM((NT, 256, hid_cols), BF16), pltpu.VMEM((NT, 256, hid_cols), BF16), pltpu.VMEM((NT, hid_cols, 256), BF16)] * 2,
            pltpu.VMEM((NKV, 16, QW), BF16),
            pltpu.VMEM((NKV, 16, QW), BF16),
            pltpu.VMEM((16 * NKV, 16 * NKV), BF16),
            pltpu.VMEM((16 * NKV, 16 * NKV), BF16),
            pltpu.VMEM((512, QW), BF16),
            pltpu.VMEM((NKV, 16, QW), BF16),
            *[pltpu.VMEM((NY, NZ, 16, QW), BF16), pltpu.VMEM((NZ, 16, QW), BF16), pltpu.VMEM((NZ, 16, QW), BF16)] * 2,
            pltpu.VMEM((16, QW), BF16),
            pltpu.VMEM((NT, 16, QW), BF16),
            pltpu.VMEM((NT, 16, QW), BF16),
            pltpu.VMEM((NT, 16, QW), BF16),
            pltpu.VMEM((NT, 16, GROUP), BF16),
            pltpu.VMEM((NT, 16, GROUP), BF16),
            pltpu.VMEM((D, 256), BF16),
            pltpu.VMEM((D, 256), BF16),
            pltpu.VMEM((D, 128), BF16),
            pltpu.VMEM((D, 128), BF16),
            pltpu.VMEM((D, 4), BF16),
            pltpu.VMEM((256, D), BF16),
            pltpu.VMEM((SEQ, GROUP, STATE), F32),
            pltpu.VMEM((SEQ, GROUP, STATE), BF16),
            pltpu.VMEM((SEQ, D), BF16),
            pltpu.VMEM((32, QW), F32),
            dma((14,)),
            dma((NT,)), dma((NT,)),
            dma((6, 7)), dma((6, 7)),
            dma((2, NY, NZ)), dma((2, NY, NZ)),
            dma((2, NY, NZ)), dma((2, NY, NZ)),
            dma((2, NZ)), dma((2, NZ)),
            dma((NT,)), dma((NT,)),
            dma((NT,)), dma((NT,)),
            dma((NT,)), dma((NT,)),
        ],
        compiler_params=pltpu.CompilerParams(
            collective_id=0, has_side_effects=True, vmem_limit_bytes=56 * 1024 * 1024
        ),
        name="layer",
    )(
        msg, mgain, par, conv,
        first_gate, first_lift, first_down, second_gate, second_lift, second_down,
        proj_gate, proj_input, proj_write, proj_read, proj_step, proj_output, scan,
    )
    heads = scan_state.shape[1]
    state_out = (
        retain[:, ::HEAD_DIM][:, :, None, None] * scan_state
        + u.reshape(SEQ, heads, HEAD_DIM)[..., None] * bc[:, None, None, :]
    )
    return out, state_out


def solution(mesh):
    placed = (
        P("kv", "tp"), P("tp"), P("tp", "kv"), P("tp", "kv"), P("kv", "tp"), P(),
        P(None, "tp"), P(None, "tp"), P(None, "tp"), P(None, "tp"), P(None, "tp"),
        P("tp"), P("tp"), P("tp"), P(None, "tp"), P(None, "tp"), P(None, "tp"),
        P("kv", None, "tp"), P("kv", None, "tp"), P("kv", None, "tp"), P("kv", "tp", None, None),
        P("tp"), P("tp", None), P("tp"), P("tp", "kv"), P("tp", "kv"), P("kv", "tp"),
    )
    return jax.shard_map(
        per_device,
        mesh=mesh,
        in_specs=placed,
        out_specs=(P("kv", "tp"), P("kv", "tp", None, None)),
        check_vma=False,
    )
```

```python
import jax
import jax.numpy as jnp
from jax import lax
from jax.experimental import pallas as pl
from jax.experimental.pallas import tpu as pltpu
from jax.sharding import PartitionSpec as P

D = 2048
HEAD_DIM = 64
STATE = 128
EPS = 1e-06

NZ, NY, NT = 8, 4, 8
NKV = NZ * NY
RPT = 4
QW = 512
SEQ = 32
GROUP = 256
MESH = pl.DeviceIdType.MESH
F32, BF16 = jnp.float32, jnp.bfloat16


def dot(a, b):
    return jnp.dot(a, b, preferred_element_type=F32)


def dot_nt(a, b):
    return lax.dot_general(a, b, (((1,), (1,)), ((), ())), preferred_element_type=F32)


def iota2(shape, dim):
    return lax.broadcasted_iota(jnp.int32, shape, dim)


def gather_rows(n):
    shape = (16 * n, 16 * n)
    row, col = iota2(shape, 0), iota2(shape, 1)
    q, rest = row // (4 * n), row % (4 * n)
    return (col == (rest // 4) * 16 + q * 4 + rest % 4).astype(BF16)


def scatter_rows(n):
    shape = (16 * n, 16 * n)
    row, col = iota2(shape, 0), iota2(shape, 1)
    q, rest = col // (4 * n), col % (4 * n)
    return (row == (rest // 4) * 16 + q * 4 + rest % 4).astype(BF16)


def piece_factor(piece):
    partial = jnp.sum(piece * piece, axis=1, keepdims=True)
    same = (iota2((16, 16), 0) % 4 == iota2((16, 16), 1) % 4).astype(F32)
    total = jnp.dot(
        same,
        jnp.broadcast_to(partial, (16, 128)),
        preferred_element_type=F32,
        precision=lax.Precision.HIGHEST,
    )
    return lax.rsqrt(total[:, :1] / D + EPS)


def kernel(
    res_ref, gain1_ref, gain2_ref, mgain_ref, ggain_ref, bias_ref, rate_ref, skip_ref,
    tapi_ref, tapw_ref, tapr_ref, bufi_ref, bufw_ref, bufr_ref,
    fg_ref, fl_ref, fd_ref, sg_ref, sl_ref, sd_ref,
    pg_ref, pi_ref, pw_ref, pr_ref, ps_ref, po_ref, scan_ref,
    out_ref, state_ref,
    msg, recv_r, wg1, wl1, wd1, wg2, wl2, wd2,
    ag1, ag2, perm, permt, hid, psend, znear, ry1, rn1, zs1, rz1, ry2, rn2, zs2, rz2,
    send_f, recv_f, recv_o, send_o, send_q, recv_q,
    pgv, piv, pwv, prv, psv, pov, scan_f, scan_b, xrow, gsplit,
    loc_sem, s_all, r_t, s_w, r_wx, r_wc, r_ag, r_y, r_z,
):
    kv = lax.axis_index("kv")
    t = lax.axis_index("tp")
    z, y = kv // NY, kv % NY
    core = t % 2

    def zpeer(d):
        return lax.rem(z + d, NZ)

    def ypeer(d):
        return lax.rem(y + d, NY)

    def tpeer(d):
        return lax.rem(t + d, NT)

    def rcopy(src, dst, ssem, rsem, dev):
        return pltpu.make_async_remote_copy(
            src_ref=src, dst_ref=dst, send_sem=ssem, recv_sem=rsem, device_id=dev, device_id_type=MESH
        )

    def wait_recv(block, rsem):
        rcopy(block, block, s_all.at[0], rsem, (kv, tpeer(1))).wait_recv()

    def wait_send(block, ssem):
        rcopy(block, block, ssem, r_t.at[0], (kv, tpeer(1))).wait_send()

    def local(src, dst, k):
        copy = pltpu.make_async_copy(src, dst, loc_sem.at[k])
        copy.start()
        return copy

    for src, dst in ((fg_ref, wg1), (fl_ref, wl1), (fd_ref, wd1)):
        local(src, dst.at[t], 1)

    barrier = pltpu.get_barrier_semaphore()
    peers = [(zpeer(d) * NY + y, t) for d in range(1, NZ)]
    peers += [(z * NY + ypeer(d), t) for d in range(1, NY)]
    peers += [(kv, tpeer(d)) for d in range(1, NT)]
    for dev in peers:
        pl.semaphore_signal(barrier, inc=1, device_id=dev, device_id_type=MESH)

    def as_row(ref):
        wide = ref[...].astype(F32)
        return jnp.concatenate([wide[k : k + 1] for k in range(wide.shape[0])], axis=1)

    row, col = iota2((128, 32), 0), iota2((128, 32), 1)
    give = ((col == (row // 16) * 4 + row % 16) & (row % 16 < 4)).astype(BF16)
    kind = (iota2((128, GROUP), 0) % 16) // 4
    body = dot(give, res_ref[...])
    body = jnp.where(kind == 1, as_row(gain1_ref), jnp.where(kind == 2, as_row(gain2_ref), body))
    msg[...] = body.astype(BF16).reshape(NT, 16, GROUP)
    recv_r[t] = msg[t]

    pl.semaphore_wait(barrier, len(peers))

    def exchange_tp(block, dst, k):
        for d in range(1, NT):
            tt = tpeer(d)
            rcopy(block(tt), dst, s_all.at[k], r_t.at[k], (kv, tt)).start()

    exchange_tp(lambda tt: msg.at[tt], recv_r.at[t], 0)

    def start_weights(k, src, dst):
        for j in range(1, 4):
            tt = lax.rem(t + 2 * j, NT)
            rcopy(src, dst.at[t], s_w.at[k], r_wx.at[k], (kv, tt)).start()
        rcopy(src, dst.at[t], s_w.at[k], r_wc.at[k], (kv, t + 1 - 2 * core)).start()

    def forward_weights(k, dst):
        wait_recv(dst.at[pl.ds(0, 3)], r_wx.at[k])
        for j in range(1, 4):
            ss = lax.rem(t - 2 * j + NT, NT)
            rcopy(dst.at[ss], dst.at[ss], s_w.at[k], r_wc.at[k], (kv, t + 1 - 2 * core)).start()

    def finish_weights(k, dst):
        wait_recv(dst.at[pl.ds(0, 4)], r_wc.at[k])
        wait_send(dst.at[pl.ds(0, 7)], s_w.at[k])

    for k, (src, dst) in enumerate(((fg_ref, wg1), (fl_ref, wl1), (fd_ref, wd1))):
        start_weights(k, src, dst)

    l_mix = [
        local(pg_ref, pgv, 3), local(pi_ref, piv, 4), local(pw_ref, pwv, 5), local(pr_ref, prv, 6),
        local(ps_ref, psv, 7), local(po_ref, pov, 8), local(scan_ref, scan_f, 9),
    ]
    for src, dst in ((sg_ref, wg2), (sl_ref, wl2), (sd_ref, wd2)):
        local(src, dst.at[t], 2)

    perm[...] = gather_rows(NKV)
    permt[...] = scatter_rows(NKV)
    wait_recv(recv_r.at[pl.ds(0, NT - 1)], r_t.at[0])

    row, col = iota2((48, 64), 0), iota2((48, 64), 1)
    pick = (col == ((row % 16) // 4) * 16 + (row // 16) * 4 + row % 4).astype(BF16)
    halves = []
    for h in range(2):
        block = jnp.concatenate([recv_r[2 * q + h] for q in range(4)], axis=0)
        halves.append(dot(pick, block))
    both = jnp.concatenate(halves, axis=1)
    res1 = both[0:16]
    gsplit[...] = both[16:48]

    ag_order = ((2, 0), (6, 0), (0, 1), (0, 3), (3, 0), (5, 0), (0, 2), (4, 0))

    def gather_send(ag, slot, f, d, e, dev):
        k = ag_order.index((d, e)) if (d, e) in ag_order else 8
        rcopy(ag.at[slot], ag.at[slot], s_all.at[4 + f], r_ag.at[f, k], (dev, t)).start()

    def start_gather(ag, f):
        for d in (4, 3, 5, 2, 6, 1, 7):
            gather_send(ag, kv, f, d, 0, zpeer(d) * NY + y)
        for e in (2, 1, 3):
            gather_send(ag, kv, f, 0, e, z * NY + ypeer(e))

    def forward_gather(ag, f):
        for k, (d, e) in enumerate(ag_order):
            slot = lax.rem(z - d + NZ, NZ) * NY + lax.rem(y - e + NY, NY)
            wait_recv(ag.at[slot], r_ag.at[f, k])
            if e == 0:
                for ee in (2, 1, 3):
                    gather_send(ag, slot, f, d, ee, z * NY + ypeer(ee))
            else:
                for dd in (1, 7):
                    gather_send(ag, slot, f, dd, e, zpeer(dd) * NY + y)

    def finish_gather(ag, f):
        wait_recv(ag.at[pl.ds(0, 23)], r_ag.at[f, 8])
        wait_send(ag.at[pl.ds(0, 31)], s_all.at[4 + f])

    def feed_forward(ag, wg, wl, wd):
        flat = ag[...].reshape(16 * NKV, QW)
        lhs = dot(perm[...], flat).astype(BF16)
        gate, lift = None, None
        for s in range(NT):
            q, h = s // 2, s % 2
            part = lhs[128 * q : 128 * q + 128, 256 * h : 256 * h + 256]
            g, u = dot_nt(part, wg[s]), dot_nt(part, wl[s])
            gate = g if gate is None else gate + g
            lift = u if lift is None else lift + u
        hidden = (gate * jax.nn.sigmoid(gate) * lift).astype(BF16)
        for s in range(NT):
            q, h = s // 2, s % 2
            hid[128 * q : 128 * q + 128, 256 * h : 256 * h + 256] = dot(hidden, wd[s]).astype(BF16)
        psend[...] = dot(permt[...], hid[...]).astype(BF16).reshape(NKV, 16, QW)

    y_order = (4, 3, 5, 2, 6, 0)

    def reduce_send_y(block, ry, f, d):
        for e in (2, 1, 3):
            yy = ypeer(e)
            k = y_order.index(d)
            rcopy(block(yy), ry.at[d, e], s_all.at[6 + f], r_y.at[f, k], (z * NY + yy, t)).start()

    def reduce_start(ry, rn, f):
        for d in (4, 3, 5, 2, 6):
            zz = zpeer(d)
            reduce_send_y(lambda yy: psend.at[zz * NY + yy], ry, f, d)
            if d == 4:
                for k, dd in enumerate((1, 7)):
                    near = zpeer(dd)
                    rcopy(
                        psend.at[pl.ds(near * NY, NY)], rn.at[pl.ds(NY * k, NY)], s_all.at[6 + f], r_z.at[f, 0],
                        (near * NY + y, t),
                    ).start()

    def reduce_finish(ry, rn, zs, rz, f):
        wait_recv(rn.at[pl.ds(0, 2 * NY)], r_z.at[f, 0])
        near = psend[pl.ds(z * NY, NY)].astype(F32) + rn[0:NY].astype(F32) + rn[NY : 2 * NY].astype(F32)
        znear[...] = near.astype(BF16)
        reduce_send_y(lambda yy: znear.at[yy], ry, f, 0)

        def with_y(total, d):
            wait_recv(ry.at[d, pl.ds(1, NY - 1)], r_y.at[f, y_order.index(d)])
            for e in range(1, NY):
                total = total + ry[d, e].astype(F32)
            return total

        for d in (4, 3, 5, 2, 6):
            zz = zpeer(d)
            zs[d] = with_y(psend[zz * NY + y].astype(F32), d).astype(BF16)
            rcopy(zs.at[d], rz.at[d], s_all.at[6 + f], r_z.at[f, 1], (zz * NY + y, t)).start()
        own = with_y(znear[y].astype(F32), 0)
        wait_recv(rz.at[pl.ds(0, 5)], r_z.at[f, 1])
        for d in (2, 6, 3, 5, 4):
            own = own + rz[d].astype(F32)
        wait_send(psend.at[pl.ds(0, 31)], s_all.at[6 + f])
        return own

    ag1[kv] = (res1 * piece_factor(res1) * gsplit[0:16]).astype(BF16)
    start_gather(ag1, 0)
    forward_gather(ag1, 0)
    for k, dst in enumerate((wg1, wl1, wd1)):
        forward_weights(k, dst)
    finish_gather(ag1, 0)
    pltpu.make_async_copy(wg1.at[pl.ds(0, 3)], wg1.at[pl.ds(0, 3)], loc_sem.at[1]).wait()
    for k, dst in enumerate((wg1, wl1, wd1)):
        finish_weights(k, dst)
    feed_forward(ag1, wg1, wl1, wd1)
    reduce_start(ry1, rn1, 0)
    start_weights(3, sg_ref, wg2)
    start_weights(4, sl_ref, wl2)
    for copy in l_mix:
        copy.wait()
    scan_b[...] = scan_f[...].astype(BF16)
    branch = reduce_finish(ry1, rn1, zs1, rz1, 0)
    first = (res1 + 0.5 * branch).astype(BF16).astype(F32)

    row, col = iota2((16, 16), 0), iota2((16, 16), 1)
    mixer_gain = jnp.concatenate(
        [dot((col == (row // 4) * 4 + j).astype(BF16), mgain_ref[...]) for j in range(4)], axis=1
    )
    send_f[...] = (first * piece_factor(first) * mixer_gain).astype(BF16)
    exchange_tp(lambda tt: send_f, recv_f.at[t], 1)
    recv_f[t] = send_f[...]
    perm8 = gather_rows(NT)
    wait_recv(recv_f.at[pl.ds(0, NT - 1)], r_t.at[1])
    rows = dot(perm8, recv_f[...].reshape(128, QW)).astype(BF16)
    for q in range(4):
        xrow[:, QW * q : QW * q + QW] = rows[32 * q : 32 * q + 32]
    mixed_in = xrow[...]

    def project(w):
        return dot(mixed_in, w[...]).astype(BF16).astype(F32)

    gate_z, input_new = project(pgv), project(piv)
    write_new, read_new, step_raw4 = project(pwv), project(prv), dot_nt(mixed_in, psv[...]).astype(BF16).astype(F32)

    def silu(v):
        return v * jax.nn.sigmoid(v)

    def short_conv(tap_ref, buf_ref, newest):
        taps = tap_ref[...].astype(F32)
        total = newest * taps[3:4]
        for k in range(3):
            total = total + buf_ref[k].astype(F32) * taps[k : k + 1]
        return silu(total)

    xc = short_conv(tapi_ref, bufi_ref, input_new)
    bc = short_conv(tapw_ref, bufw_ref, write_new)
    rc = short_conv(tapr_ref, bufr_ref, read_new)
    lane_head = iota2((SEQ, GROUP), 1) // HEAD_DIM
    step_raw = jnp.zeros((SEQ, GROUP), F32)
    for h in range(4):
        step_raw = jnp.where(lane_head == h, step_raw4[:, h : h + 1], step_raw)
    head_row = iota2((1, GROUP), 1) // HEAD_DIM

    def per_head(ref):
        wide = jnp.full((1, GROUP), ref[0], F32)
        for h in range(1, 4):
            wide = jnp.where(head_row == h, ref[h], wide)
        return wide

    pre = step_raw + per_head(bias_ref)
    step = jnp.maximum(pre, 0.0) + jnp.log1p(jnp.exp(-jnp.abs(pre)))
    retain = jnp.exp(-step * jnp.exp(per_head(rate_ref)))
    u = step * xc
    rcb = rc.astype(BF16)
    sub = iota2((8, GROUP), 0)
    reads = []
    for g in range(4):
        acc = jnp.zeros((8, GROUP), F32)
        for j in range(8):
            b = 8 * g + j
            got = dot_nt(rcb[8 * g : 8 * g + 8], scan_b[b])
            acc = jnp.where(sub == j, got, acc)
        reads.append(acc)
    read = jnp.concatenate(reads, axis=0)
    head = retain * read + u * jnp.sum(bc * rc, axis=1, keepdims=True) + per_head(skip_ref) * xc
    gated = head.astype(BF16).astype(F32) * silu(gate_z)
    gated = gated * lax.rsqrt(jnp.mean(gated * gated, axis=1, keepdims=True) + EPS) * as_row(ggain_ref)
    part = dot(gated.astype(BF16), pov[...]).astype(BF16)
    stacked = jnp.concatenate([part[:, QW * q : QW * q + QW] for q in range(4)], axis=0)
    send_o[...] = dot(scatter_rows(NT), stacked).astype(BF16).reshape(NT, 16, QW)
    exchange_tp(lambda tt: send_o.at[tt], recv_o.at[t], 2)
    recv_o[t] = send_o[t]
    pltpu.make_async_copy(wg2.at[pl.ds(0, 3)], wg2.at[pl.ds(0, 3)], loc_sem.at[2]).wait()
    start_weights(5, sd_ref, wd2)
    u_cols = jnp.transpose(u)
    for b in range(SEQ):
        for h in range(4):
            rows_h = slice(HEAD_DIM * h, HEAD_DIM * h + HEAD_DIM)
            keep = jnp.broadcast_to(retain[b : b + 1, HEAD_DIM * h : HEAD_DIM * h + 1], (HEAD_DIM, STATE))
            scan_f[b, rows_h, :] = keep * scan_f[b, rows_h, :] + u_cols[rows_h, b : b + 1] * bc[b : b + 1]
    l_state = local(scan_f, state_ref, 0)
    wait_recv(recv_o.at[pl.ds(0, NT - 1)], r_t.at[2])
    mixed = first
    for k in range(NT):
        mixed = mixed + recv_o[k].astype(F32)
    res2 = mixed.astype(BF16).astype(F32)

    ag2[kv] = (res2 * piece_factor(res2) * gsplit[16:32]).astype(BF16)
    start_gather(ag2, 1)
    forward_weights(3, wg2)
    forward_weights(4, wl2)
    forward_gather(ag2, 1)
    forward_weights(5, wd2)
    finish_gather(ag2, 1)
    for k, dst in enumerate((wg2, wl2, wd2)):
        finish_weights(3 + k, dst)
    feed_forward(ag2, wg2, wl2, wd2)
    reduce_start(ry2, rn2, 1)
    branch = reduce_finish(ry2, rn2, zs2, rz2, 1)
    final = (res2 + 0.5 * branch).astype(BF16)

    row, col = iota2((64, 16), 0), iota2((64, 16), 1)
    spread = ((col == (row // 16) * 4 + row % 16) & (row % 16 < 4)).astype(BF16)
    for h in range(2):
        block = dot(spread, final[:, 256 * h : 256 * h + 256]).astype(BF16).reshape(4, 16, 256)
        for q in range(4):
            send_q[2 * q + h] = block[q]
    exchange_tp(lambda tt: send_q.at[tt], recv_q.at[t], 3)
    recv_q[t] = send_q[t]
    row, col = iota2((32, 128), 0), iota2((32, 128), 1)
    pick32 = (col == (row // 4) * 16 + row % 4).astype(BF16)
    wait_recv(recv_q.at[pl.ds(0, NT - 1)], r_t.at[3])
    out_ref[...] = dot(pick32, recv_q[...].reshape(128, 256)).astype(BF16)

    l_state.wait()
    for k, block in enumerate((recv_r, recv_f, recv_o, recv_q)):
        wait_send(block.at[pl.ds(0, NT - 1)], s_all.at[k])


def per_device(
    residual, first_gain, first_gate, first_lift, first_down, mixer_gain,
    proj_gate, proj_input, proj_write, proj_read, proj_step,
    step_bias, rate_log, skip_gain, taps_input, taps_write, taps_read,
    buffer_input, buffer_write, buffer_read, scan_state, group_gain, proj_output,
    second_gain, second_gate, second_lift, second_down,
):
    scan = scan_state.reshape(SEQ, GROUP, STATE)
    vm = pl.BlockSpec(memory_space=pltpu.VMEM)
    sm = pl.BlockSpec(memory_space=pltpu.SMEM)
    anym = pl.BlockSpec(memory_space=pl.ANY)
    hid_cols = first_gate.shape[1]
    dma = pltpu.SemaphoreType.DMA
    out, state = pl.pallas_call(
        kernel,
        out_shape=(
            pltpu.VMEM((SEQ, GROUP), BF16),
            pltpu.VMEM((SEQ, GROUP, STATE), F32),
        ),
        in_specs=[vm] * 5 + [sm] * 3 + [vm] * 6 + [anym] * 13,
        out_specs=(vm, anym),
        scratch_shapes=[
            pltpu.VMEM((NT, 16, GROUP), BF16),
            pltpu.VMEM((NT, 16, GROUP), BF16),
            *[pltpu.VMEM((NT, hid_cols, 256), BF16), pltpu.VMEM((NT, hid_cols, 256), BF16), pltpu.VMEM((NT, hid_cols, 256), BF16)] * 2,
            pltpu.VMEM((NKV, 16, QW), BF16),
            pltpu.VMEM((NKV, 16, QW), BF16),
            pltpu.VMEM((16 * NKV, 16 * NKV), BF16),
            pltpu.VMEM((16 * NKV, 16 * NKV), BF16),
            pltpu.VMEM((512, QW), BF16),
            pltpu.VMEM((NKV, 16, QW), BF16),
            pltpu.VMEM((NY, 16, QW), BF16),
            *[pltpu.VMEM((NZ, NY, 16, QW), BF16), pltpu.VMEM((2 * NY, 16, QW), BF16), pltpu.VMEM((NZ, 16, QW), BF16), pltpu.VMEM((NZ, 16, QW), BF16)] * 2,
            pltpu.VMEM((16, QW), BF16),
            pltpu.VMEM((NT, 16, QW), BF16),
            pltpu.VMEM((NT, 16, QW), BF16),
            pltpu.VMEM((NT, 16, QW), BF16),
            pltpu.VMEM((NT, 16, GROUP), BF16),
            pltpu.VMEM((NT, 16, GROUP), BF16),
            pltpu.VMEM((D, 256), BF16),
            pltpu.VMEM((D, 256), BF16),
            pltpu.VMEM((D, 128), BF16),
            pltpu.VMEM((D, 128), BF16),
            pltpu.VMEM((4, D), BF16),
            pltpu.VMEM((256, D), BF16),
            pltpu.VMEM((SEQ, GROUP, STATE), F32),
            pltpu.VMEM((SEQ, GROUP, STATE), BF16),
            pltpu.VMEM((SEQ, D), BF16),
            pltpu.VMEM((32, QW), F32),
            dma((10,)), dma((8,)), dma((4,)),
            dma((6,)), dma((6,)), dma((6,)),
            dma((2, 9)), dma((2, 6)), dma((2, 2)),
        ],
        compiler_params=pltpu.CompilerParams(
            collective_id=0, has_side_effects=True, vmem_limit_bytes=56 * 1024 * 1024
        ),
        name="layer",
    )(
        residual, first_gain.reshape(2, 128), second_gain.reshape(2, 128), mixer_gain.reshape(16, 128),
        group_gain.reshape(2, 128), step_bias, rate_log, skip_gain,
        taps_input, taps_write, taps_read,
        buffer_input.transpose(1, 0, 2), buffer_write.transpose(1, 0, 2), buffer_read.transpose(1, 0, 2),
        first_gate.T, first_lift.T, first_down, second_gate.T, second_lift.T, second_down,
        proj_gate, proj_input, proj_write, proj_read, proj_step.T, proj_output, scan,
    )
    return out, state.reshape(scan_state.shape)


def solution(mesh):
    placed = (
        P("kv", "tp"), P("tp"), P("tp", "kv"), P("tp", "kv"), P("kv", "tp"), P(),
        P(None, "tp"), P(None, "tp"), P(None, "tp"), P(None, "tp"), P(None, "tp"),
        P("tp"), P("tp"), P("tp"), P(None, "tp"), P(None, "tp"), P(None, "tp"),
        P("kv", None, "tp"), P("kv", None, "tp"), P("kv", None, "tp"), P("kv", "tp", None, None),
        P("tp"), P("tp", None), P("tp"), P("tp", "kv"), P("tp", "kv"), P("kv", "tp"),
    )
    return jax.shard_map(
        per_device,
        mesh=mesh,
        in_specs=placed,
        out_specs=(P("kv", "tp"), P("kv", "tp", None, None)),
        check_vma=False,
    )
```

```python
import jax
import jax.numpy as jnp
from jax import lax
from jax.experimental import pallas as pl
from jax.experimental.pallas import tpu as pltpu
from jax.sharding import PartitionSpec as P

D = 2048
HEAD_DIM = 64
STATE = 128
EPS = 1e-06

NZ, NY, NT = 8, 4, 8
NKV = NZ * NY
RPT = 4
QW = 512
SEQ = 32
GROUP = 256
MESH = pl.DeviceIdType.MESH
F32, BF16 = jnp.float32, jnp.bfloat16


def dot(a, b):
    return jnp.dot(a, b, preferred_element_type=F32)


def dot_nt(a, b):
    return lax.dot_general(a, b, (((1,), (1,)), ((), ())), preferred_element_type=F32)


def iota2(shape, dim):
    return lax.broadcasted_iota(jnp.int32, shape, dim)


def gather_rows(n):
    shape = (16 * n, 16 * n)
    row, col = iota2(shape, 0), iota2(shape, 1)
    q, rest = row // (4 * n), row % (4 * n)
    return (col == (rest // 4) * 16 + q * 4 + rest % 4).astype(BF16)


def scatter_rows(n):
    shape = (16 * n, 16 * n)
    row, col = iota2(shape, 0), iota2(shape, 1)
    q, rest = col // (4 * n), col % (4 * n)
    return (row == (rest // 4) * 16 + q * 4 + rest % 4).astype(BF16)


def piece_factor(piece):
    partial = jnp.sum(piece * piece, axis=1, keepdims=True)
    same = (iota2((16, 16), 0) % 4 == iota2((16, 16), 1) % 4).astype(F32)
    total = jnp.dot(
        same,
        jnp.broadcast_to(partial, (16, 128)),
        preferred_element_type=F32,
        precision=lax.Precision.HIGHEST,
    )
    return lax.rsqrt(total[:, :1] / D + EPS)


def kernel(*refs):
    small_in, refs = refs[:14], refs[14:]
    (fg_ref, fl_ref, fd_ref, sg_ref, sl_ref, sd_ref), refs = refs[:6], refs[6:]
    (pg_ref, pi_ref, pw_ref, pr_ref, ps_ref, po_ref, scan_ref), refs = refs[:7], refs[7:]
    (out_ref, state_ref), refs = refs[:2], refs[2:]
    small, refs = refs[:14], refs[14:]
    res_ref, gain1_ref, gain2_ref, mgain_ref, ggain_ref, bias_ref, rate_ref, skip_ref = small[:8]
    tapi_ref, tapw_ref, tapr_ref, bufi_ref, bufw_ref, bufr_ref = small[8:]
    (
        msg, recv_r, wg1, wl1, wd1, wg2, wl2, wd2,
        ag1, ag2, perm, permt, hid, psend, znear, ry1, rn1, zs1, rz1, ry2, rn2, zs2, rz2,
        send_f, recv_f, recv_o, send_o, send_q, recv_q,
        pgv, piv, pwv, prv, psv, pov, scan_f, scan_b, xrow, gsplit,
        loc_sem, s_all, r_t, s_w, r_wx, r_wo, r_wc, r_ag, r_y, r_z, in_sem, ready,
    ) = refs
    kv = lax.axis_index("kv")
    t = lax.axis_index("tp")
    z, y = kv // NY, kv % NY
    core = t % 2

    def zpeer(d):
        return lax.rem(z + d, NZ)

    def ypeer(d):
        return lax.rem(y + d, NY)

    def tpeer(d):
        return lax.rem(t + d, NT)

    def rcopy(src, dst, ssem, rsem, dev):
        return pltpu.make_async_remote_copy(
            src_ref=src, dst_ref=dst, send_sem=ssem, recv_sem=rsem, device_id=dev, device_id_type=MESH
        )

    def wait_recv(block, rsem):
        rcopy(block, block, s_all.at[0], rsem, (kv, tpeer(1))).wait_recv()

    def wait_send(block, ssem):
        rcopy(block, block, ssem, r_t.at[0], (kv, tpeer(1))).wait_send()

    def local(src, dst, k):
        copy = pltpu.make_async_copy(src, dst, loc_sem.at[k])
        copy.start()
        return copy

    barrier = pltpu.get_barrier_semaphore()
    peers = [(kv, tpeer(d)) for d in range(1, NT)]
    peers += [(zpeer(d) * NY + y, t) for d in (1, 7)]
    peers += [(z * NY + ypeer(d), t) for d in range(1, NY)]
    for dev in peers:
        pl.semaphore_signal(barrier, inc=1, device_id=dev, device_id_type=MESH)
    l_small = []
    for k in range(14):
        copy = pltpu.make_async_copy(small_in[k], small[k], in_sem.at[k])
        copy.start()
        l_small.append(copy)
    for src, dst in ((fg_ref, wg1), (fl_ref, wl1), (fd_ref, wd1)):
        local(src, dst.at[t], 1)
    for k in range(3):
        l_small[k].wait()

    def as_row(ref):
        wide = ref[...].astype(F32)
        return jnp.concatenate([wide[k : k + 1] for k in range(wide.shape[0])], axis=1)

    row, col = iota2((128, 32), 0), iota2((128, 32), 1)
    give = ((col == (row // 16) * 4 + row % 16) & (row % 16 < 4)).astype(BF16)
    kind = (iota2((128, GROUP), 0) % 16) // 4
    body = dot(give, res_ref[...])
    body = jnp.where(kind == 1, as_row(gain1_ref), jnp.where(kind == 2, as_row(gain2_ref), body))
    msg[...] = body.astype(BF16).reshape(NT, 16, GROUP)
    recv_r[t] = msg[t]

    pl.semaphore_wait(barrier, len(peers))

    def exchange_tp(block, dst, k):
        for d in range(1, NT):
            tt = tpeer(d)
            rcopy(block(tt), dst, s_all.at[k], r_t.at[k], (kv, tt)).start()

    exchange_tp(lambda tt: msg.at[tt], recv_r.at[t], 0)
    for d in (1, 7):
        pl.semaphore_signal(ready.at[0], inc=1, device_id=(zpeer(d) * NY + y, t), device_id_type=MESH)

    partner = t + 1 - 2 * core
    left, right, across = lax.rem(t + NT - 2, NT), lax.rem(t + 2, NT), lax.rem(t + 4, NT)
    cuts = (fg_ref.shape[0], 0, 96)

    def start_weights(k, src, dst):
        for tt in (right, left):
            rcopy(src, dst.at[t], s_w.at[k], r_wx.at[k], (kv, tt)).start()
        rcopy(src, dst.at[t], s_w.at[k], r_wc.at[k], (kv, partner)).start()

    def relay_weights(k, dst):
        wait_recv(dst.at[pl.ds(0, 2)], r_wx.at[k])
        cut, depth = cuts[k % 3], dst.shape[1]
        if cut > 0:
            part = dst.at[left, pl.ds(0, cut)]
            rcopy(part, part, s_w.at[k], r_wo.at[k], (kv, right)).start()
        if cut < depth:
            part = dst.at[right, pl.ds(cut, depth - cut)]
            rcopy(part, part, s_w.at[k], r_wo.at[k], (kv, left)).start()
        for ss in (left, right):
            rcopy(dst.at[ss], dst.at[ss], s_w.at[k], r_wc.at[k], (kv, partner)).start()

    def forward_weights(k, dst):
        wait_recv(dst.at[0], r_wo.at[k])
        rcopy(dst.at[across], dst.at[across], s_w.at[k], r_wc.at[k], (kv, partner)).start()

    def finish_weights(k, dst):
        wait_recv(dst.at[pl.ds(0, 4)], r_wc.at[k])
        wait_send(dst.at[pl.ds(0, 7)], s_w.at[k])

    for k, (src, dst) in enumerate(((fg_ref, wg1), (fl_ref, wl1), (fd_ref, wd1))):
        start_weights(k, src, dst)

    l_mix = [
        local(pg_ref, pgv, 3), local(pi_ref, piv, 4), local(pw_ref, pwv, 5), local(pr_ref, prv, 6),
        local(ps_ref, psv, 7), local(po_ref, pov, 8), local(scan_ref, scan_f, 9),
    ]
    for src, dst in ((sg_ref, wg2), (sl_ref, wl2), (sd_ref, wd2)):
        local(src, dst.at[t], 2)

    pl.semaphore_wait(ready.at[0], 2)
    for d in (2, 6):
        pl.semaphore_signal(ready.at[1], inc=1, device_id=(zpeer(d) * NY + y, t), device_id_type=MESH)
    perm[...] = gather_rows(NKV)
    permt[...] = scatter_rows(NKV)
    for k in range(3, 14):
        l_small[k].wait()
    wait_recv(recv_r.at[pl.ds(0, NT - 1)], r_t.at[0])

    pl.semaphore_wait(ready.at[1], 2)
    row, col = iota2((48, 64), 0), iota2((48, 64), 1)
    pick = (col == ((row % 16) // 4) * 16 + (row // 16) * 4 + row % 4).astype(BF16)
    halves = []
    for h in range(2):
        block = jnp.concatenate([recv_r[2 * q + h] for q in range(4)], axis=0)
        halves.append(dot(pick, block))
    both = jnp.concatenate(halves, axis=1)
    res1 = both[0:16]
    gsplit[...] = both[16:48]

    ag_order = ((2, 0), (6, 0), (0, 1), (0, 3), (3, 0), (5, 0), (0, 2), (4, 0))

    def gather_send(ag, slot, f, d, e, dev):
        k = ag_order.index((d, e)) if (d, e) in ag_order else 8
        rcopy(ag.at[slot], ag.at[slot], s_all.at[4 + f], r_ag.at[f, k], (dev, t)).start()

    def start_gather(ag, f):
        for d in (4, 3, 5, 2, 6, 1, 7):
            gather_send(ag, kv, f, d, 0, zpeer(d) * NY + y)
        for e in (2, 1, 3):
            gather_send(ag, kv, f, 0, e, z * NY + ypeer(e))

    def forward_gather(ag, f, between=()):
        for k, (d, e) in enumerate(ag_order):
            for at, step, weights in between:
                if at == k:
                    relay_weights(step, weights)
            slot = lax.rem(z - d + NZ, NZ) * NY + lax.rem(y - e + NY, NY)
            wait_recv(ag.at[slot], r_ag.at[f, k])
            if e == 0:
                for ee in (2, 1, 3):
                    gather_send(ag, slot, f, d, ee, z * NY + ypeer(ee))
            else:
                for dd in (1, 7):
                    gather_send(ag, slot, f, dd, e, zpeer(dd) * NY + y)

    def finish_gather(ag, f):
        wait_recv(ag.at[pl.ds(0, 23)], r_ag.at[f, 8])
        wait_send(ag.at[pl.ds(0, 31)], s_all.at[4 + f])

    def feed_forward(ag, wg, wl, wd, k):
        flat = ag[...].reshape(16 * NKV, QW)
        lhs = dot(perm[...], flat).astype(BF16)
        gate, lift = None, None
        for s in range(NT):
            q, h = s // 2, s % 2
            part = lhs[128 * q : 128 * q + 128, 256 * h : 256 * h + 256]
            g, u = dot_nt(part, wg[s]), dot_nt(part, wl[s])
            gate = g if gate is None else gate + g
            lift = u if lift is None else lift + u
        finish_weights(k + 2, wd)
        hidden = (gate * jax.nn.sigmoid(gate) * lift).astype(BF16)
        for s in range(NT):
            q, h = s // 2, s % 2
            hid[128 * q : 128 * q + 128, 256 * h : 256 * h + 256] = dot(hidden, wd[s]).astype(BF16)
        psend[...] = dot(permt[...], hid[...]).astype(BF16).reshape(NKV, 16, QW)

    y_order = (4, 3, 5, 2, 6, 0)

    def reduce_send_y(block, ry, f, d):
        for e in (2, 1, 3):
            yy = ypeer(e)
            k = y_order.index(d)
            rcopy(block(yy), ry.at[d, e], s_all.at[6 + f], r_y.at[f, k], (z * NY + yy, t)).start()

    def reduce_start(ry, rn, f):
        for d in (4, 3, 5, 2, 6):
            zz = zpeer(d)
            reduce_send_y(lambda yy: psend.at[zz * NY + yy], ry, f, d)
            if d == 4:
                for k, dd in enumerate((1, 7)):
                    near = zpeer(dd)
                    rcopy(
                        psend.at[pl.ds(near * NY, NY)], rn.at[pl.ds(NY * k, NY)], s_all.at[6 + f], r_z.at[f, 0],
                        (near * NY + y, t),
                    ).start()

    def reduce_finish(ry, rn, zs, rz, f, between=()):
        wait_recv(rn.at[pl.ds(0, 2 * NY)], r_z.at[f, 0])
        near = psend[pl.ds(z * NY, NY)].astype(F32) + rn[0:NY].astype(F32) + rn[NY : 2 * NY].astype(F32)
        znear[...] = near.astype(BF16)
        reduce_send_y(lambda yy: znear.at[yy], ry, f, 0)

        def with_y(total, d):
            wait_recv(ry.at[d, pl.ds(1, NY - 1)], r_y.at[f, y_order.index(d)])
            for e in range(1, NY):
                total = total + ry[d, e].astype(F32)
            return total

        for d in (4, 3, 5, 2, 6):
            for at, step, weights in between:
                if at == d:
                    relay_weights(step, weights)
            zz = zpeer(d)
            zs[d] = with_y(psend[zz * NY + y].astype(F32), d).astype(BF16)
            rcopy(zs.at[d], rz.at[d], s_all.at[6 + f], r_z.at[f, 1], (zz * NY + y, t)).start()
        own = with_y(znear[y].astype(F32), 0)
        wait_recv(rz.at[pl.ds(0, 5)], r_z.at[f, 1])
        for d in (2, 6, 3, 5, 4):
            own = own + rz[d].astype(F32)
        wait_send(psend.at[pl.ds(0, 31)], s_all.at[6 + f])
        return own

    ag1[kv] = (res1 * piece_factor(res1) * gsplit[0:16]).astype(BF16)
    start_gather(ag1, 0)
    forward_gather(ag1, 0, ((0, 0, wg1), (0, 1, wl1), (4, 2, wd1)))
    for k, dst in enumerate((wg1, wl1, wd1)):
        forward_weights(k, dst)
    for k, (src, dst) in enumerate(((sg_ref, wg2), (sl_ref, wl2), (sd_ref, wd2))):
        start_weights(3 + k, src, dst)
    finish_gather(ag1, 0)
    pltpu.make_async_copy(wg1.at[pl.ds(0, 3)], wg1.at[pl.ds(0, 3)], loc_sem.at[1]).wait()
    finish_weights(0, wg1)
    finish_weights(1, wl1)
    feed_forward(ag1, wg1, wl1, wd1, 0)
    reduce_start(ry1, rn1, 0)
    for copy in l_mix:
        copy.wait()
    scan_b[...] = scan_f[...].astype(BF16)
    branch = reduce_finish(ry1, rn1, zs1, rz1, 0, ((4, 3, wg2), (4, 4, wl2), (5, 5, wd2)))
    first = (res1 + 0.5 * branch).astype(BF16).astype(F32)

    row, col = iota2((16, 16), 0), iota2((16, 16), 1)
    mixer_gain = jnp.concatenate(
        [dot((col == (row // 4) * 4 + j).astype(BF16), mgain_ref[...]) for j in range(4)], axis=1
    )
    send_f[...] = (first * piece_factor(first) * mixer_gain).astype(BF16)
    exchange_tp(lambda tt: send_f, recv_f.at[t], 1)
    recv_f[t] = send_f[...]
    perm8 = gather_rows(NT)
    wait_recv(recv_f.at[pl.ds(0, NT - 1)], r_t.at[1])
    for k, dst in enumerate((wg2, wl2, wd2)):
        forward_weights(3 + k, dst)
    rows = dot(perm8, recv_f[...].reshape(128, QW)).astype(BF16)
    for q in range(4):
        xrow[:, QW * q : QW * q + QW] = rows[32 * q : 32 * q + 32]
    mixed_in = xrow[...]

    def project(w):
        return dot(mixed_in, w[...]).astype(BF16).astype(F32)

    gate_z, input_new = project(pgv), project(piv)
    write_new, read_new, step_raw4 = project(pwv), project(prv), dot_nt(mixed_in, psv[...]).astype(BF16).astype(F32)

    def silu(v):
        return v * jax.nn.sigmoid(v)

    def short_conv(tap_ref, buf_ref, newest):
        taps = tap_ref[...].astype(F32)
        total = newest * taps[3:4]
        for k in range(3):
            total = total + buf_ref[k].astype(F32) * taps[k : k + 1]
        return silu(total)

    xc = short_conv(tapi_ref, bufi_ref, input_new)
    bc = short_conv(tapw_ref, bufw_ref, write_new)
    rc = short_conv(tapr_ref, bufr_ref, read_new)
    lane_head = iota2((SEQ, GROUP), 1) // HEAD_DIM
    step_raw = jnp.zeros((SEQ, GROUP), F32)
    for h in range(4):
        step_raw = jnp.where(lane_head == h, step_raw4[:, h : h + 1], step_raw)
    head_row = iota2((1, GROUP), 1) // HEAD_DIM

    def per_head(ref):
        values = ref[...]
        wide = jnp.broadcast_to(values[:, 0:1], (1, GROUP))
        for h in range(1, 4):
            wide = jnp.where(head_row == h, values[:, h : h + 1], wide)
        return wide

    pre = step_raw + per_head(bias_ref)
    step = jnp.maximum(pre, 0.0) + jnp.log1p(jnp.exp(-jnp.abs(pre)))
    retain = jnp.exp(-step * jnp.exp(per_head(rate_ref)))
    u = step * xc
    rcb = rc.astype(BF16)
    sub = iota2((8, GROUP), 0)
    reads = []
    for g in range(4):
        acc = jnp.zeros((8, GROUP), F32)
        for j in range(8):
            b = 8 * g + j
            got = dot_nt(rcb[8 * g : 8 * g + 8], scan_b[b])
            acc = jnp.where(sub == j, got, acc)
        reads.append(acc)
    read = jnp.concatenate(reads, axis=0)
    head = retain * read + u * jnp.sum(bc * rc, axis=1, keepdims=True) + per_head(skip_ref) * xc
    gated = head.astype(BF16).astype(F32) * silu(gate_z)
    gated = gated * lax.rsqrt(jnp.mean(gated * gated, axis=1, keepdims=True) + EPS) * as_row(ggain_ref)
    part = dot(gated.astype(BF16), pov[...]).astype(BF16)
    stacked = jnp.concatenate([part[:, QW * q : QW * q + QW] for q in range(4)], axis=0)
    send_o[...] = dot(scatter_rows(NT), stacked).astype(BF16).reshape(NT, 16, QW)
    exchange_tp(lambda tt: send_o.at[tt], recv_o.at[t], 2)
    recv_o[t] = send_o[t]
    pltpu.make_async_copy(wg2.at[pl.ds(0, 3)], wg2.at[pl.ds(0, 3)], loc_sem.at[2]).wait()
    u_cols = jnp.transpose(u)
    for b in range(SEQ):
        for h in range(4):
            rows_h = slice(HEAD_DIM * h, HEAD_DIM * h + HEAD_DIM)
            keep = jnp.broadcast_to(retain[b : b + 1, HEAD_DIM * h : HEAD_DIM * h + 1], (HEAD_DIM, STATE))
            scan_f[b, rows_h, :] = keep * scan_f[b, rows_h, :] + u_cols[rows_h, b : b + 1] * bc[b : b + 1]
    l_state = local(scan_f, state_ref, 0)
    wait_recv(recv_o.at[pl.ds(0, NT - 1)], r_t.at[2])
    mixed = first
    for k in range(NT):
        mixed = mixed + recv_o[k].astype(F32)
    res2 = mixed.astype(BF16).astype(F32)

    ag2[kv] = (res2 * piece_factor(res2) * gsplit[16:32]).astype(BF16)
    start_gather(ag2, 1)
    forward_gather(ag2, 1)
    finish_gather(ag2, 1)
    finish_weights(3, wg2)
    finish_weights(4, wl2)
    feed_forward(ag2, wg2, wl2, wd2, 3)
    reduce_start(ry2, rn2, 1)
    branch = reduce_finish(ry2, rn2, zs2, rz2, 1)
    final = (res2 + 0.5 * branch).astype(BF16)

    row, col = iota2((64, 16), 0), iota2((64, 16), 1)
    spread = ((col == (row // 16) * 4 + row % 16) & (row % 16 < 4)).astype(BF16)
    for h in range(2):
        block = dot(spread, final[:, 256 * h : 256 * h + 256]).astype(BF16).reshape(4, 16, 256)
        for q in range(4):
            send_q[2 * q + h] = block[q]
    exchange_tp(lambda tt: send_q.at[tt], recv_q.at[t], 3)
    recv_q[t] = send_q[t]
    row, col = iota2((32, 128), 0), iota2((32, 128), 1)
    pick32 = (col == (row // 4) * 16 + row % 4).astype(BF16)
    wait_recv(recv_q.at[pl.ds(0, NT - 1)], r_t.at[3])
    out_ref[...] = dot(pick32, recv_q[...].reshape(128, 256)).astype(BF16)

    l_state.wait()
    for k, block in enumerate((recv_r, recv_f, recv_o, recv_q)):
        wait_send(block.at[pl.ds(0, NT - 1)], s_all.at[k])


def per_device(
    residual, first_gain, first_gate, first_lift, first_down, mixer_gain,
    proj_gate, proj_input, proj_write, proj_read, proj_step,
    step_bias, rate_log, skip_gain, taps_input, taps_write, taps_read,
    buffer_input, buffer_write, buffer_read, scan_state, group_gain, proj_output,
    second_gain, second_gate, second_lift, second_down,
):
    scan = scan_state.reshape(SEQ, GROUP, STATE)
    anym = pl.BlockSpec(memory_space=pl.ANY)
    hid_cols = first_gate.shape[1]
    dma = pltpu.SemaphoreType.DMA
    small = (
        residual, first_gain.reshape(2, 128), second_gain.reshape(2, 128), mixer_gain.reshape(16, 128),
        group_gain.reshape(2, 128), step_bias.reshape(1, 4), rate_log.reshape(1, 4), skip_gain.reshape(1, 4),
        taps_input, taps_write, taps_read,
        buffer_input.transpose(1, 0, 2), buffer_write.transpose(1, 0, 2), buffer_read.transpose(1, 0, 2),
    )
    out, state = pl.pallas_call(
        kernel,
        out_shape=(
            pltpu.VMEM((SEQ, GROUP), BF16),
            pltpu.VMEM((SEQ, GROUP, STATE), F32),
        ),
        in_specs=[anym] * 27,
        out_specs=(pl.BlockSpec(memory_space=pltpu.VMEM), anym),
        scratch_shapes=[
            *[pltpu.VMEM(a.shape, a.dtype) for a in small],
            pltpu.VMEM((NT, 16, GROUP), BF16),
            pltpu.VMEM((NT, 16, GROUP), BF16),
            *[pltpu.VMEM((NT, hid_cols, 256), BF16), pltpu.VMEM((NT, hid_cols, 256), BF16), pltpu.VMEM((NT, hid_cols, 256), BF16)] * 2,
            pltpu.VMEM((NKV, 16, QW), BF16),
            pltpu.VMEM((NKV, 16, QW), BF16),
            pltpu.VMEM((16 * NKV, 16 * NKV), BF16),
            pltpu.VMEM((16 * NKV, 16 * NKV), BF16),
            pltpu.VMEM((512, QW), BF16),
            pltpu.VMEM((NKV, 16, QW), BF16),
            pltpu.VMEM((NY, 16, QW), BF16),
            *[pltpu.VMEM((NZ, NY, 16, QW), BF16), pltpu.VMEM((2 * NY, 16, QW), BF16), pltpu.VMEM((NZ, 16, QW), BF16), pltpu.VMEM((NZ, 16, QW), BF16)] * 2,
            pltpu.VMEM((16, QW), BF16),
            pltpu.VMEM((NT, 16, QW), BF16),
            pltpu.VMEM((NT, 16, QW), BF16),
            pltpu.VMEM((NT, 16, QW), BF16),
            pltpu.VMEM((NT, 16, GROUP), BF16),
            pltpu.VMEM((NT, 16, GROUP), BF16),
            pltpu.VMEM((D, 256), BF16),
            pltpu.VMEM((D, 256), BF16),
            pltpu.VMEM((D, 128), BF16),
            pltpu.VMEM((D, 128), BF16),
            pltpu.VMEM((4, D), BF16),
            pltpu.VMEM((256, D), BF16),
            pltpu.VMEM((SEQ, GROUP, STATE), F32),
            pltpu.VMEM((SEQ, GROUP, STATE), BF16),
            pltpu.VMEM((SEQ, D), BF16),
            pltpu.VMEM((32, QW), F32),
            dma((10,)), dma((8,)), dma((4,)),
            dma((6,)), dma((6,)), dma((6,)), dma((6,)),
            dma((2, 9)), dma((2, 6)), dma((2, 2)), dma((14,)), pltpu.SemaphoreType.REGULAR((2,)),
        ],
        compiler_params=pltpu.CompilerParams(
            collective_id=0, has_side_effects=True, vmem_limit_bytes=56 * 1024 * 1024
        ),
        name="layer",
    )(
        *small,
        first_gate.T, first_lift.T, first_down, second_gate.T, second_lift.T, second_down,
        proj_gate, proj_input, proj_write, proj_read, proj_step.T, proj_output, scan,
    )
    return out, state.reshape(scan_state.shape)


def solution(mesh):
    placed = (
        P("kv", "tp"), P("tp"), P("tp", "kv"), P("tp", "kv"), P("kv", "tp"), P(),
        P(None, "tp"), P(None, "tp"), P(None, "tp"), P(None, "tp"), P(None, "tp"),
        P("tp"), P("tp"), P("tp"), P(None, "tp"), P(None, "tp"), P(None, "tp"),
        P("kv", None, "tp"), P("kv", None, "tp"), P("kv", None, "tp"), P("kv", "tp", None, None),
        P("tp"), P("tp", None), P("tp"), P("tp", "kv"), P("tp", "kv"), P("kv", "tp"),
    )
    return jax.shard_map(
        per_device,
        mesh=mesh,
        in_specs=placed,
        out_specs=(P("kv", "tp"), P("kv", "tp", None, None)),
        check_vma=False,
    )
```

```python
import jax
import jax.numpy as jnp
from jax import lax
from jax.experimental import pallas as pl
from jax.experimental.pallas import tpu as pltpu
from jax.sharding import PartitionSpec as P

D = 2048
HEAD_DIM = 64
STATE = 128
EPS = 1e-06

NZ, NY, NT = 8, 4, 8
NKV = NZ * NY
RPT = 4
QW = 512
SEQ = 32
GROUP = 256
MESH = pl.DeviceIdType.MESH
F32, BF16 = jnp.float32, jnp.bfloat16


def dot(a, b):
    return jnp.dot(a, b, preferred_element_type=F32)


def dot_nt(a, b):
    return lax.dot_general(a, b, (((1,), (1,)), ((), ())), preferred_element_type=F32)


def iota2(shape, dim):
    return lax.broadcasted_iota(jnp.int32, shape, dim)


def gather_rows(n):
    shape = (16 * n, 16 * n)
    row, col = iota2(shape, 0), iota2(shape, 1)
    q, rest = row // (4 * n), row % (4 * n)
    return (col == (rest // 4) * 16 + q * 4 + rest % 4).astype(BF16)


def scatter_rows(n):
    shape = (16 * n, 16 * n)
    row, col = iota2(shape, 0), iota2(shape, 1)
    q, rest = col // (4 * n), col % (4 * n)
    return (row == (rest // 4) * 16 + q * 4 + rest % 4).astype(BF16)


def piece_factor(piece):
    square = piece * piece
    total = square[:, 0:128] + square[:, 128:256] + square[:, 256:384] + square[:, 384:512]
    total = total + pltpu.roll(total, 8, 0)
    total = total + pltpu.roll(total, 4, 0)
    return lax.rsqrt(jnp.sum(total, axis=1, keepdims=True) / D + EPS)


def kernel(*refs):
    small_in, refs = refs[:14], refs[14:]
    (fg_ref, fl_ref, fd_ref, sg_ref, sl_ref, sd_ref), refs = refs[:6], refs[6:]
    (pg_ref, pi_ref, pw_ref, pr_ref, ps_ref, po_ref, scan_ref), refs = refs[:7], refs[7:]
    (out_ref, state_ref), refs = refs[:2], refs[2:]
    small, refs = refs[:14], refs[14:]
    res_ref, gain1_ref, gain2_ref, mgain_ref, ggain_ref, bias_ref, rate_ref, skip_ref = small[:8]
    tapi_ref, tapw_ref, tapr_ref, bufi_ref, bufw_ref, bufr_ref = small[8:]
    (
        msg, recv_r, wg1, wl1, wd1, wg2, wl2, wd2,
        ag1, ag2, perm, permt, lhs_v, hid, psend, znear, ry1, rn1, zs1, rz1, ry2, rn2, zs2, rz2,
        send_f, recv_f, recv_o, send_o, send_q, recv_q,
        pgv, piv, pwv, prv, psv, pov, scan_f, scan_b, xrow, gsplit,
        loc_sem, s_all, r_t, s_w, r_wx, r_wo, r_wc, r_ag, r_y, r_z, in_sem, ready,
    ) = refs
    kv = lax.axis_index("kv")
    t = lax.axis_index("tp")
    z, y = kv // NY, kv % NY
    core = t % 2

    def zpeer(d):
        return lax.rem(z + d, NZ)

    def ypeer(d):
        return lax.rem(y + d, NY)

    def tpeer(d):
        return lax.rem(t + d, NT)

    def rcopy(src, dst, ssem, rsem, dev):
        return pltpu.make_async_remote_copy(
            src_ref=src, dst_ref=dst, send_sem=ssem, recv_sem=rsem, device_id=dev, device_id_type=MESH
        )

    def wait_recv(block, rsem):
        rcopy(block, block, s_all.at[0], rsem, (kv, tpeer(1))).wait_recv()

    def wait_send(block, ssem):
        rcopy(block, block, ssem, r_t.at[0], (kv, tpeer(1))).wait_send()

    def local(src, dst, k):
        copy = pltpu.make_async_copy(src, dst, loc_sem.at[k])
        copy.start()
        return copy

    barrier = pltpu.get_barrier_semaphore()
    peers = [(kv, tpeer(d)) for d in range(1, NT)]
    peers += [(zpeer(d) * NY + y, t) for d in (1, 7)]
    peers += [(z * NY + ypeer(d), t) for d in range(1, NY)]
    for dev in peers:
        pl.semaphore_signal(barrier, inc=1, device_id=dev, device_id_type=MESH)
    l_small = []
    for k in range(14):
        copy = pltpu.make_async_copy(small_in[k], small[k], in_sem.at[k])
        copy.start()
        l_small.append(copy)
    for src, dst in ((fg_ref, wg1), (fl_ref, wl1), (fd_ref, wd1)):
        local(src, dst.at[t], 1)
    for k in range(3):
        l_small[k].wait()

    def as_row(ref):
        wide = ref[...].astype(F32)
        return jnp.concatenate([wide[k : k + 1] for k in range(wide.shape[0])], axis=1)

    row, col = iota2((128, 32), 0), iota2((128, 32), 1)
    give = ((col == (row // 16) * 4 + row % 16) & (row % 16 < 4)).astype(BF16)
    kind = (iota2((128, GROUP), 0) % 16) // 4
    body = dot(give, res_ref[...])
    body = jnp.where(kind == 1, as_row(gain1_ref), jnp.where(kind == 2, as_row(gain2_ref), body))
    msg[...] = body.astype(BF16).reshape(NT, 16, GROUP)
    recv_r[t] = msg[t]

    pl.semaphore_wait(barrier, len(peers))

    def exchange_tp(block, dst, k):
        base = t - core
        far, right, left = lax.rem(base + 4, NT), lax.rem(base + 2, NT), lax.rem(base + 6, NT)
        for tt in (far, far + 1, right, left, right + 1, left + 1, base + 1 - core):
            rcopy(block(tt), dst, s_all.at[k], r_t.at[k], (kv, tt)).start()

    exchange_tp(lambda tt: msg.at[tt], recv_r.at[t], 0)
    for d in (1, 7):
        pl.semaphore_signal(ready.at[0], inc=1, device_id=(zpeer(d) * NY + y, t), device_id_type=MESH)

    partner = t + 1 - 2 * core
    left, right, across = lax.rem(t + NT - 2, NT), lax.rem(t + 2, NT), lax.rem(t + 4, NT)
    cuts = (fg_ref.shape[0], 0, 96)

    def start_weights(k, src, dst):
        for tt in (right, left):
            rcopy(src, dst.at[t], s_w.at[k], r_wx.at[k], (kv, tt)).start()
        rcopy(src, dst.at[t], s_w.at[k], r_wc.at[k], (kv, partner)).start()

    def relay_weights(k, dst):
        wait_recv(dst.at[pl.ds(0, 2)], r_wx.at[k])
        cut, depth = cuts[k % 3], dst.shape[1]
        if cut > 0:
            part = dst.at[left, pl.ds(0, cut)]
            rcopy(part, part, s_w.at[k], r_wo.at[k], (kv, right)).start()
        if cut < depth:
            part = dst.at[right, pl.ds(cut, depth - cut)]
            rcopy(part, part, s_w.at[k], r_wo.at[k], (kv, left)).start()
        for ss in (left, right):
            rcopy(dst.at[ss], dst.at[ss], s_w.at[k], r_wc.at[k], (kv, partner)).start()

    def forward_weights(k, dst):
        wait_recv(dst.at[0], r_wo.at[k])
        rcopy(dst.at[across], dst.at[across], s_w.at[k], r_wc.at[k], (kv, partner)).start()

    def finish_weights(k, dst):
        wait_recv(dst.at[pl.ds(0, 4)], r_wc.at[k])
        wait_send(dst.at[pl.ds(0, 7)], s_w.at[k])

    for k, (src, dst) in enumerate(((fg_ref, wg1), (fl_ref, wl1), (fd_ref, wd1))):
        start_weights(k, src, dst)

    l_mix = [
        local(pg_ref, pgv, 3), local(pi_ref, piv, 4), local(pw_ref, pwv, 5), local(pr_ref, prv, 6),
        local(ps_ref, psv, 7), local(po_ref, pov, 8), local(scan_ref, scan_f, 9),
    ]
    for src, dst in ((sg_ref, wg2), (sl_ref, wl2), (sd_ref, wd2)):
        local(src, dst.at[t], 2)

    pl.semaphore_wait(ready.at[0], 2)
    for d in (2, 6):
        pl.semaphore_signal(ready.at[1], inc=1, device_id=(zpeer(d) * NY + y, t), device_id_type=MESH)
    perm[...] = gather_rows(NT)
    permt[...] = scatter_rows(NT)
    for k in range(3, 14):
        l_small[k].wait()
    wait_recv(recv_r.at[pl.ds(0, NT - 1)], r_t.at[0])

    pl.semaphore_wait(ready.at[1], 2)
    row, col = iota2((48, 64), 0), iota2((48, 64), 1)
    pick = (col == ((row % 16) // 4) * 16 + (row // 16) * 4 + row % 4).astype(BF16)
    halves = []
    for h in range(2):
        block = jnp.concatenate([recv_r[2 * q + h] for q in range(4)], axis=0)
        halves.append(dot(pick, block))
    both = jnp.concatenate(halves, axis=1)
    res1 = both[0:16]
    gsplit[...] = both[16:48]

    ag_order = ((2, 0), (6, 0), (0, 1), (0, 3), (3, 0), (5, 0), (0, 2), (4, 0))

    def gather_send(ag, slot, f, d, e, dev):
        k = ag_order.index((d, e)) if (d, e) in ag_order else 8
        rcopy(ag.at[slot], ag.at[slot], s_all.at[4], r_ag.at[k], (dev, t)).start()

    def start_gather(ag, f):
        for d in (4, 3, 5, 2, 6, 1, 7):
            gather_send(ag, kv, f, d, 0, zpeer(d) * NY + y)
        for e in (2, 1, 3):
            gather_send(ag, kv, f, 0, e, z * NY + ypeer(e))

    def forward_gather(ag, f, between=()):
        for k, (d, e) in enumerate(ag_order):
            for at, step, weights in between:
                if at == k:
                    relay_weights(step, weights)
            slot = lax.rem(z - d + NZ, NZ) * NY + lax.rem(y - e + NY, NY)
            wait_recv(ag.at[slot], r_ag.at[k])
            if e == 0:
                for ee in (2, 1, 3):
                    gather_send(ag, slot, f, d, ee, z * NY + ypeer(ee))
            else:
                for dd in (1, 7):
                    gather_send(ag, slot, f, dd, e, zpeer(dd) * NY + y)

    def finish_gather(ag, f):
        wait_recv(ag.at[pl.ds(0, 23)], r_ag.at[8])
        wait_send(ag.at[pl.ds(0, 31)], s_all.at[4])

    def feed_forward(ag, wg, wl, wd, k):
        for g in range(NKV // 8):
            rows = dot(perm[...], ag[8 * g : 8 * g + 8].reshape(128, QW)).astype(BF16)
            for q in range(4):
                lhs_v[q, 32 * g : 32 * g + 32] = rows[32 * q : 32 * q + 32]
        gate, lift = None, None
        for s in range(NT):
            q, h = s // 2, s % 2
            part = lhs_v[q, :, 256 * h : 256 * h + 256]
            g, u = dot_nt(part, wg[s]), dot_nt(part, wl[s])
            gate = g if gate is None else gate + g
            lift = u if lift is None else lift + u
        finish_weights(k + 2, wd)
        hidden = (gate * jax.nn.sigmoid(gate) * lift).astype(BF16)
        for s in range(NT):
            q, h = s // 2, s % 2
            out = dot(hidden, wd[s]).astype(BF16)
            for g in range(NKV // 8):
                hid[g, 32 * q : 32 * q + 32, 256 * h : 256 * h + 256] = out[32 * g : 32 * g + 32]
        for g in range(NKV // 8):
            psend[8 * g : 8 * g + 8] = dot(permt[...], hid[g]).astype(BF16).reshape(8, 16, QW)

    y_order = (4, 3, 5, 2, 6, 0)

    def reduce_send_y(block, ry, f, d):
        for e in (2, 1, 3):
            yy = ypeer(e)
            k = y_order.index(d)
            rcopy(block(yy), ry.at[d, e], s_all.at[5], r_y.at[k], (z * NY + yy, t)).start()

    def reduce_start(ry, rn, f):
        for d in (4, 3, 5, 2, 6):
            zz = zpeer(d)
            reduce_send_y(lambda yy: psend.at[zz * NY + yy], ry, f, d)
            if d == 4:
                for k, dd in enumerate((1, 7)):
                    near = zpeer(dd)
                    rcopy(
                        psend.at[pl.ds(near * NY, NY)], rn.at[pl.ds(NY * k, NY)], s_all.at[5], r_z.at[0],
                        (near * NY + y, t),
                    ).start()

    def reduce_finish(ry, rn, zs, rz, f, between=()):
        def with_y(total, d):
            wait_recv(ry.at[d, pl.ds(1, NY - 1)], r_y.at[y_order.index(d)])
            for e in range(1, NY):
                total = total + ry[d, e].astype(F32)
            return total

        for d in (4, 3, 5, 2, 6):
            zz = zpeer(d)
            zs[d] = with_y(psend[zz * NY + y].astype(F32), d).astype(BF16)
            rcopy(zs.at[d], rz.at[d], s_all.at[5], r_z.at[1], (zz * NY + y, t)).start()
            if d == 4:
                wait_recv(rn.at[pl.ds(0, 2 * NY)], r_z.at[0])
                near = psend[pl.ds(z * NY, NY)].astype(F32) + rn[0:NY].astype(F32) + rn[NY : 2 * NY].astype(F32)
                znear[...] = near.astype(BF16)
                reduce_send_y(lambda yy: znear.at[yy], ry, f, 0)
            for at, step, weights in between:
                if at == d:
                    relay_weights(step, weights)
        own = with_y(znear[y].astype(F32), 0)
        wait_recv(rz.at[pl.ds(0, 5)], r_z.at[1])
        for d in (2, 6, 3, 5, 4):
            own = own + rz[d].astype(F32)
        wait_send(psend.at[pl.ds(0, 31)], s_all.at[5])
        return own

    ag1[kv] = (res1 * piece_factor(res1) * gsplit[0:16]).astype(BF16)
    start_gather(ag1, 0)
    forward_gather(ag1, 0, ((0, 0, wg1), (0, 1, wl1), (4, 2, wd1)))
    for k, dst in enumerate((wg1, wl1, wd1)):
        forward_weights(k, dst)
    for k, (src, dst) in enumerate(((sg_ref, wg2), (sl_ref, wl2), (sd_ref, wd2))):
        start_weights(3 + k, src, dst)
    finish_gather(ag1, 0)
    pltpu.make_async_copy(wg1.at[pl.ds(0, 3)], wg1.at[pl.ds(0, 3)], loc_sem.at[1]).wait()
    finish_weights(0, wg1)
    finish_weights(1, wl1)
    feed_forward(ag1, wg1, wl1, wd1, 0)
    reduce_start(ry1, rn1, 0)
    for copy in l_mix:
        copy.wait()
    scan_b[...] = scan_f[...].astype(BF16)
    branch = reduce_finish(ry1, rn1, zs1, rz1, 0, ((4, 3, wg2), (4, 4, wl2), (5, 5, wd2)))
    first = (res1 + 0.5 * branch).astype(BF16).astype(F32)

    row, col = iota2((16, 16), 0), iota2((16, 16), 1)
    mixer_gain = jnp.concatenate(
        [dot((col == (row // 4) * 4 + j).astype(BF16), mgain_ref[...]) for j in range(4)], axis=1
    )
    send_f[...] = (first * piece_factor(first) * mixer_gain).astype(BF16)
    exchange_tp(lambda tt: send_f, recv_f.at[t], 1)
    recv_f[t] = send_f[...]
    def silu(v):
        return v * jax.nn.sigmoid(v)

    def old_taps(tap_ref, buf_ref):
        taps = tap_ref[...].astype(F32)
        total = buf_ref[0].astype(F32) * taps[0:1]
        for k in range(1, 3):
            total = total + buf_ref[k].astype(F32) * taps[k : k + 1]
        return total, taps[3:4]

    conv_i, conv_w, conv_r = old_taps(tapi_ref, bufi_ref), old_taps(tapw_ref, bufw_ref), old_taps(tapr_ref, bufr_ref)
    head_row = iota2((1, GROUP), 1) // HEAD_DIM

    def per_head(ref):
        values = ref[...]
        wide = jnp.broadcast_to(values[:, 0:1], (1, GROUP))
        for h in range(1, 4):
            wide = jnp.where(head_row == h, values[:, h : h + 1], wide)
        return wide

    bias_row, rate_row, skip_row = per_head(bias_ref), jnp.exp(per_head(rate_ref)), per_head(skip_ref)
    ggain_row = as_row(ggain_ref)
    wait_recv(recv_f.at[pl.ds(0, NT - 1)], r_t.at[1])
    for k, dst in enumerate((wg2, wl2, wd2)):
        forward_weights(3 + k, dst)
    rows = dot(perm[...], recv_f[...].reshape(128, QW)).astype(BF16)
    for q in range(4):
        xrow[:, QW * q : QW * q + QW] = rows[32 * q : 32 * q + 32]
    mixed_in = xrow[...]

    def project(w):
        return dot(mixed_in, w[...]).astype(BF16).astype(F32)

    gate_z, input_new = project(pgv), project(piv)
    write_new, read_new, step_raw4 = project(pwv), project(prv), dot_nt(mixed_in, psv[...]).astype(BF16).astype(F32)

    xc = silu(conv_i[0] + input_new * conv_i[1])
    bc = silu(conv_w[0] + write_new * conv_w[1])
    rc = silu(conv_r[0] + read_new * conv_r[1])
    lane_head = iota2((SEQ, GROUP), 1) // HEAD_DIM
    step_raw = jnp.zeros((SEQ, GROUP), F32)
    for h in range(4):
        step_raw = jnp.where(lane_head == h, step_raw4[:, h : h + 1], step_raw)
    pre = step_raw + bias_row
    step = jnp.maximum(pre, 0.0) + jnp.log1p(jnp.exp(-jnp.abs(pre)))
    retain = jnp.exp(-step * rate_row)
    u = step * xc
    rcb = rc.astype(BF16)
    sub = iota2((8, GROUP), 0)
    reads = []
    for g in range(4):
        acc = jnp.zeros((8, GROUP), F32)
        for j in range(8):
            b = 8 * g + j
            got = dot_nt(rcb[8 * g : 8 * g + 8], scan_b[b])
            acc = jnp.where(sub == j, got, acc)
        reads.append(acc)
    read = jnp.concatenate(reads, axis=0)
    head = retain * read + u * jnp.sum(bc * rc, axis=1, keepdims=True) + skip_row * xc
    gated = head.astype(BF16).astype(F32) * silu(gate_z)
    gated = gated * lax.rsqrt(jnp.mean(gated * gated, axis=1, keepdims=True) + EPS) * ggain_row
    part = dot(gated.astype(BF16), pov[...]).astype(BF16)
    stacked = jnp.concatenate([part[:, QW * q : QW * q + QW] for q in range(4)], axis=0)
    send_o[...] = dot(permt[...], stacked).astype(BF16).reshape(NT, 16, QW)
    exchange_tp(lambda tt: send_o.at[tt], recv_o.at[t], 2)
    recv_o[t] = send_o[t]
    pltpu.make_async_copy(wg2.at[pl.ds(0, 3)], wg2.at[pl.ds(0, 3)], loc_sem.at[2]).wait()
    u_cols = jnp.transpose(u)
    for b in range(SEQ):
        for h in range(4):
            rows_h = slice(HEAD_DIM * h, HEAD_DIM * h + HEAD_DIM)
            keep = jnp.broadcast_to(retain[b : b + 1, HEAD_DIM * h : HEAD_DIM * h + 1], (HEAD_DIM, STATE))
            scan_f[b, rows_h, :] = keep * scan_f[b, rows_h, :] + u_cols[rows_h, b : b + 1] * bc[b : b + 1]
    l_state = local(scan_f, state_ref, 0)
    wait_recv(recv_o.at[pl.ds(0, NT - 1)], r_t.at[2])
    mixed = first
    for k in range(NT):
        mixed = mixed + recv_o[k].astype(F32)
    res2 = mixed.astype(BF16).astype(F32)

    ag2[kv] = (res2 * piece_factor(res2) * gsplit[16:32]).astype(BF16)
    start_gather(ag2, 1)
    forward_gather(ag2, 1)
    finish_gather(ag2, 1)
    finish_weights(3, wg2)
    finish_weights(4, wl2)
    feed_forward(ag2, wg2, wl2, wd2, 3)
    reduce_start(ry2, rn2, 1)
    branch = reduce_finish(ry2, rn2, zs2, rz2, 1)
    final = (res2 + 0.5 * branch).astype(BF16)

    row, col = iota2((64, 16), 0), iota2((64, 16), 1)
    spread = ((col == (row // 16) * 4 + row % 16) & (row % 16 < 4)).astype(BF16)
    for h in range(2):
        block = dot(spread, final[:, 256 * h : 256 * h + 256]).astype(BF16).reshape(4, 16, 256)
        for q in range(4):
            send_q[2 * q + h] = block[q]
    exchange_tp(lambda tt: send_q.at[tt], recv_q.at[t], 3)
    recv_q[t] = send_q[t]
    row, col = iota2((32, 128), 0), iota2((32, 128), 1)
    pick32 = (col == (row // 4) * 16 + row % 4).astype(BF16)
    wait_recv(recv_q.at[pl.ds(0, NT - 1)], r_t.at[3])
    out_ref[...] = dot(pick32, recv_q[...].reshape(128, 256)).astype(BF16)

    l_state.wait()
    for k, block in enumerate((recv_r, recv_f, recv_o, recv_q)):
        wait_send(block.at[pl.ds(0, NT - 1)], s_all.at[k])


def per_device(
    residual, first_gain, first_gate, first_lift, first_down, mixer_gain,
    proj_gate, proj_input, proj_write, proj_read, proj_step,
    step_bias, rate_log, skip_gain, taps_input, taps_write, taps_read,
    buffer_input, buffer_write, buffer_read, scan_state, group_gain, proj_output,
    second_gain, second_gate, second_lift, second_down,
):
    scan = scan_state.reshape(SEQ, GROUP, STATE)
    anym = pl.BlockSpec(memory_space=pl.ANY)
    hid_cols = first_gate.shape[1]
    dma = pltpu.SemaphoreType.DMA
    small = (
        residual, first_gain.reshape(2, 128), second_gain.reshape(2, 128), mixer_gain.reshape(16, 128),
        group_gain.reshape(2, 128), step_bias.reshape(1, 4), rate_log.reshape(1, 4), skip_gain.reshape(1, 4),
        taps_input, taps_write, taps_read,
        buffer_input.transpose(1, 0, 2), buffer_write.transpose(1, 0, 2), buffer_read.transpose(1, 0, 2),
    )
    out, state = pl.pallas_call(
        kernel,
        out_shape=(
            pltpu.VMEM((SEQ, GROUP), BF16),
            pltpu.VMEM((SEQ, GROUP, STATE), F32),
        ),
        in_specs=[anym] * 27,
        out_specs=(pl.BlockSpec(memory_space=pltpu.VMEM), anym),
        scratch_shapes=[
            *[pltpu.VMEM(a.shape, a.dtype) for a in small],
            pltpu.VMEM((NT, 16, GROUP), BF16),
            pltpu.VMEM((NT, 16, GROUP), BF16),
            *[pltpu.VMEM((NT, hid_cols, 256), BF16), pltpu.VMEM((NT, hid_cols, 256), BF16), pltpu.VMEM((NT, hid_cols, 256), BF16)] * 2,
            pltpu.VMEM((NKV, 16, QW), BF16),
            pltpu.VMEM((NKV, 16, QW), BF16),
            pltpu.VMEM((128, 128), BF16),
            pltpu.VMEM((128, 128), BF16),
            pltpu.VMEM((4, 128, QW), BF16),
            pltpu.VMEM((4, 128, QW), BF16),
            pltpu.VMEM((NKV, 16, QW), BF16),
            pltpu.VMEM((NY, 16, QW), BF16),
            *[pltpu.VMEM((NZ, NY, 16, QW), BF16), pltpu.VMEM((2 * NY, 16, QW), BF16), pltpu.VMEM((NZ, 16, QW), BF16), pltpu.VMEM((NZ, 16, QW), BF16)] * 2,
            pltpu.VMEM((16, QW), BF16),
            pltpu.VMEM((NT, 16, QW), BF16),
            pltpu.VMEM((NT, 16, QW), BF16),
            pltpu.VMEM((NT, 16, QW), BF16),
            pltpu.VMEM((NT, 16, GROUP), BF16),
            pltpu.VMEM((NT, 16, GROUP), BF16),
            pltpu.VMEM((D, 256), BF16),
            pltpu.VMEM((D, 256), BF16),
            pltpu.VMEM((D, 128), BF16),
            pltpu.VMEM((D, 128), BF16),
            pltpu.VMEM((4, D), BF16),
            pltpu.VMEM((256, D), BF16),
            pltpu.VMEM((SEQ, GROUP, STATE), F32),
            pltpu.VMEM((SEQ, GROUP, STATE), BF16),
            pltpu.VMEM((SEQ, D), BF16),
            pltpu.VMEM((32, QW), F32),
            dma((10,)), dma((6,)), dma((4,)),
            dma((6,)), dma((6,)), dma((6,)), dma((6,)),
            dma((9,)), dma((6,)), dma((2,)), dma((14,)), pltpu.SemaphoreType.REGULAR((2,)),
        ],
        compiler_params=pltpu.CompilerParams(
            collective_id=0, has_side_effects=True, vmem_limit_bytes=56 * 1024 * 1024
        ),
        name="layer",
    )(
        *small,
        first_gate.T, first_lift.T, first_down, second_gate.T, second_lift.T, second_down,
        proj_gate, proj_input, proj_write, proj_read, proj_step.T, proj_output, scan,
    )
    return out, state.reshape(scan_state.shape)


def solution(mesh):
    placed = (
        P("kv", "tp"), P("tp"), P("tp", "kv"), P("tp", "kv"), P("kv", "tp"), P(),
        P(None, "tp"), P(None, "tp"), P(None, "tp"), P(None, "tp"), P(None, "tp"),
        P("tp"), P("tp"), P("tp"), P(None, "tp"), P(None, "tp"), P(None, "tp"),
        P("kv", None, "tp"), P("kv", None, "tp"), P("kv", None, "tp"), P("kv", "tp", None, None),
        P("tp"), P("tp", None), P("tp"), P("tp", "kv"), P("tp", "kv"), P("kv", "tp"),
    )
    return jax.shard_map(
        per_device,
        mesh=mesh,
        in_specs=placed,
        out_specs=(P("kv", "tp"), P("kv", "tp", None, None)),
        check_vma=False,
    )
```

```python
import jax
import jax.numpy as jnp
from jax import lax
from jax.experimental import pallas as pl
from jax.experimental.pallas import tpu as pltpu
from jax.sharding import PartitionSpec as P

D = 2048
HEAD_DIM = 64
STATE = 128
EPS = 1e-06

NZ, NY, NT = 8, 4, 8
NKV = NZ * NY
RPT = 4
QW = 512
SEQ = 32
GROUP = 256
MESH = pl.DeviceIdType.MESH
F32, BF16 = jnp.float32, jnp.bfloat16


def dot(a, b):
    return jnp.dot(a, b, preferred_element_type=F32)


def dot_nt(a, b):
    return lax.dot_general(a, b, (((1,), (1,)), ((), ())), preferred_element_type=F32)


def iota2(shape, dim):
    return lax.broadcasted_iota(jnp.int32, shape, dim)


def gather_rows(n):
    shape = (16 * n, 16 * n)
    row, col = iota2(shape, 0), iota2(shape, 1)
    q, rest = row // (4 * n), row % (4 * n)
    return (col == (rest // 4) * 16 + q * 4 + rest % 4).astype(BF16)


def scatter_rows(n):
    shape = (16 * n, 16 * n)
    row, col = iota2(shape, 0), iota2(shape, 1)
    q, rest = col // (4 * n), col % (4 * n)
    return (row == (rest // 4) * 16 + q * 4 + rest % 4).astype(BF16)


def piece_factor(piece):
    square = piece * piece
    total = square[:, 0:128] + square[:, 128:256] + square[:, 256:384] + square[:, 384:512]
    total = total + pltpu.roll(total, 8, 0)
    total = total + pltpu.roll(total, 4, 0)
    return lax.rsqrt(jnp.sum(total, axis=1, keepdims=True) / D + EPS)


def kernel(*refs):
    small_in, refs = refs[:14], refs[14:]
    (fg_ref, fl_ref, fd_ref, sg_ref, sl_ref, sd_ref), refs = refs[:6], refs[6:]
    (pg_ref, pi_ref, pw_ref, pr_ref, ps_ref, po_ref, scan_ref), refs = refs[:7], refs[7:]
    (out_ref, state_ref), refs = refs[:2], refs[2:]
    small, refs = refs[:14], refs[14:]
    res_ref, gain1_ref, gain2_ref, mgain_ref, ggain_ref, bias_ref, rate_ref, skip_ref = small[:8]
    tapi_ref, tapw_ref, tapr_ref, bufi_ref, bufw_ref, bufr_ref = small[8:]
    (
        msg, recv_r, up1, down1, up2, down2,
        ag1, ag2, perm, permt, lhs_v, hid, psend, znear, ry1, rn1, zs1, rz1, ry2, rn2, zs2, rz2,
        send_f, recv_f, recv_o, send_o, send_q, recv_q,
        pgi, pwr, psv, pov, scan_f, scan_b, xrow, gsplit,
        loc_sem, s_all, r_t, s_w, r_wx, r_wo, r_wc, r_ag, r_y, r_z, in_sem, ready,
    ) = refs
    kv = lax.axis_index("kv")
    t = lax.axis_index("tp")
    z, y = kv // NY, kv % NY
    core = t % 2

    def zpeer(d):
        return lax.rem(z + d, NZ)

    def ypeer(d):
        return lax.rem(y + d, NY)

    def tpeer(d):
        return lax.rem(t + d, NT)

    def rcopy(src, dst, ssem, rsem, dev):
        return pltpu.make_async_remote_copy(
            src_ref=src, dst_ref=dst, send_sem=ssem, recv_sem=rsem, device_id=dev, device_id_type=MESH
        )

    def wait_recv(block, rsem):
        rcopy(block, block, s_all.at[0], rsem, (kv, tpeer(1))).wait_recv()

    def wait_send(block, ssem):
        rcopy(block, block, ssem, r_t.at[0], (kv, tpeer(1))).wait_send()

    def local(src, dst, k):
        copy = pltpu.make_async_copy(src, dst, loc_sem.at[k])
        copy.start()
        return copy

    barrier = pltpu.get_barrier_semaphore()
    peers = [(kv, tpeer(d)) for d in range(1, NT)]
    peers += [(zpeer(d) * NY + y, t) for d in (1, 7)]
    peers += [(z * NY + ypeer(d), t) for d in range(1, NY)]
    for dev in peers:
        pl.semaphore_signal(barrier, inc=1, device_id=dev, device_id_type=MESH)
    l_small = []
    for k in range(14):
        copy = pltpu.make_async_copy(small_in[k], small[k], in_sem.at[k])
        copy.start()
        l_small.append(copy)
    hid_units = fg_ref.shape[0]
    sources = (fg_ref, fl_ref, fd_ref, sg_ref, sl_ref, sd_ref)
    gathered = ((up1, 0), (up1, hid_units), (down1, 0), (up2, 0), (up2, hid_units), (down2, 0))

    def block_of(k, s, first=0, rows=None):
        dst, top = gathered[k]
        return dst.at[pl.ds(top + first, rows or hid_units), pl.ds(pl.multiple_of(s * 256, 256), 256)]

    def bytes_of(k, count):
        dst, top = gathered[k]
        return dst.at[pl.ds(top, hid_units), pl.ds(0, 256 * count)]

    for k in range(3):
        local(sources[k], block_of(k, t), 1)
    for k in range(3):
        l_small[k].wait()

    def as_row(ref):
        wide = ref[...].astype(F32)
        return jnp.concatenate([wide[k : k + 1] for k in range(wide.shape[0])], axis=1)

    row, col = iota2((128, 32), 0), iota2((128, 32), 1)
    give = ((col == (row // 16) * 4 + row % 16) & (row % 16 < 4)).astype(BF16)
    kind = (iota2((128, GROUP), 0) % 16) // 4
    body = dot(give, res_ref[...])
    body = jnp.where(kind == 1, as_row(gain1_ref), jnp.where(kind == 2, as_row(gain2_ref), body))
    msg[...] = body.astype(BF16).reshape(NT, 16, GROUP)
    recv_r[t] = msg[t]

    pl.semaphore_wait(barrier, len(peers))

    def exchange_tp(block, dst, k):
        base = t - core
        far, right, left = lax.rem(base + 4, NT), lax.rem(base + 2, NT), lax.rem(base + 6, NT)
        for tt in (far, far + 1, right, left, right + 1, left + 1, base + 1 - core):
            rcopy(block(tt), dst, s_all.at[k], r_t.at[k], (kv, tt)).start()

    exchange_tp(lambda tt: msg.at[tt], recv_r.at[t], 0)
    for d in (1, 7):
        pl.semaphore_signal(ready.at[0], inc=1, device_id=(zpeer(d) * NY + y, t), device_id_type=MESH)

    partner = t + 1 - 2 * core
    left, right, across = lax.rem(t + NT - 2, NT), lax.rem(t + 2, NT), lax.rem(t + 4, NT)
    cuts = (hid_units, 0, 96)

    def start_weights(k):
        for tt in (right, left):
            rcopy(sources[k], block_of(k, t), s_w.at[k], r_wx.at[k], (kv, tt)).start()
        rcopy(sources[k], block_of(k, t), s_w.at[k], r_wc.at[k], (kv, partner)).start()

    def relay_weights(k):
        wait_recv(bytes_of(k, 2), r_wx.at[k])
        cut = cuts[k % 3]
        if cut > 0:
            part = block_of(k, left, 0, cut)
            rcopy(part, part, s_w.at[k], r_wo.at[k], (kv, right)).start()
        if cut < hid_units:
            part = block_of(k, right, cut, hid_units - cut)
            rcopy(part, part, s_w.at[k], r_wo.at[k], (kv, left)).start()
        for ss in (left, right):
            rcopy(block_of(k, ss), block_of(k, ss), s_w.at[k], r_wc.at[k], (kv, partner)).start()

    def forward_weights(k):
        wait_recv(bytes_of(k, 1), r_wo.at[k])
        rcopy(block_of(k, across), block_of(k, across), s_w.at[k], r_wc.at[k], (kv, partner)).start()

    def finish_weights(k):
        wait_recv(bytes_of(k, 4), r_wc.at[k])
        wait_send(bytes_of(k, 7), s_w.at[k])

    for k in range(3):
        start_weights(k)

    l_mix = [
        local(pg_ref, pgi.at[:, pl.ds(0, 256)], 3), local(pi_ref, pgi.at[:, pl.ds(256, 256)], 4),
        local(pw_ref, pwr.at[:, pl.ds(0, 128)], 5), local(pr_ref, pwr.at[:, pl.ds(128, 128)], 6),
        local(ps_ref, psv, 7), local(po_ref, pov, 8), local(scan_ref, scan_f, 9),
    ]
    for k in range(3, 6):
        local(sources[k], block_of(k, t), 2)

    pl.semaphore_wait(ready.at[0], 2)
    for d in (2, 6):
        pl.semaphore_signal(ready.at[1], inc=1, device_id=(zpeer(d) * NY + y, t), device_id_type=MESH)
    perm[...] = gather_rows(NT)
    permt[...] = scatter_rows(NT)
    for k in range(3, 14):
        l_small[k].wait()
    wait_recv(recv_r.at[pl.ds(0, NT - 1)], r_t.at[0])

    pl.semaphore_wait(ready.at[1], 2)
    row, col = iota2((48, 64), 0), iota2((48, 64), 1)
    pick = (col == ((row % 16) // 4) * 16 + (row // 16) * 4 + row % 4).astype(BF16)
    halves = []
    for h in range(2):
        block = jnp.concatenate([recv_r[2 * q + h] for q in range(4)], axis=0)
        halves.append(dot(pick, block))
    both = jnp.concatenate(halves, axis=1)
    res1 = both[0:16]
    gsplit[...] = both[16:48]

    ag_order = ((2, 0), (6, 0), (3, 0), (5, 0), (0, 1), (0, 3), (4, 0), (0, 2))

    def gather_send(ag, slot, f, d, e, dev):
        k = ag_order.index((d, e)) if (d, e) in ag_order else 8
        rcopy(ag.at[slot], ag.at[slot], s_all.at[4], r_ag.at[k], (dev, t)).start()

    def start_gather(ag, f):
        for d in (4, 3, 5, 2, 6, 1, 7):
            gather_send(ag, kv, f, d, 0, zpeer(d) * NY + y)
        for e in (2, 1, 3):
            gather_send(ag, kv, f, 0, e, z * NY + ypeer(e))

    def forward_gather(ag, f, between=()):
        for k, (d, e) in enumerate(ag_order):
            for at, step in between:
                if at == k:
                    relay_weights(step)
            slot = lax.rem(z - d + NZ, NZ) * NY + lax.rem(y - e + NY, NY)
            wait_recv(ag.at[slot], r_ag.at[k])
            if e == 0:
                for ee in (2, 1, 3):
                    gather_send(ag, slot, f, d, ee, z * NY + ypeer(ee))
            else:
                for dd in (1, 7):
                    gather_send(ag, slot, f, dd, e, zpeer(dd) * NY + y)

    def finish_gather(ag, f):
        wait_recv(ag.at[pl.ds(0, 23)], r_ag.at[8])
        wait_send(ag.at[pl.ds(0, 31)], s_all.at[4])

    def feed_forward(ag, up, down, k):
        for g in range(NKV // 8):
            rows = dot(perm[...], ag[8 * g : 8 * g + 8].reshape(128, QW)).astype(BF16)
            for q in range(4):
                lhs_v[32 * g : 32 * g + 32, QW * q : QW * q + QW] = rows[32 * q : 32 * q + 32]
        lhs = lhs_v[...]
        gate, lift = dot_nt(lhs, up[0:hid_units]), dot_nt(lhs, up[hid_units : 2 * hid_units])
        finish_weights(k + 2)
        hidden = (gate * jax.nn.sigmoid(gate) * lift).astype(BF16)
        out = dot(hidden, down[...]).astype(BF16)
        for g in range(NKV // 8):
            for q in range(4):
                hid[g, 32 * q : 32 * q + 32] = out[32 * g : 32 * g + 32, QW * q : QW * q + QW]
        for g in range(NKV // 8):
            psend[8 * g : 8 * g + 8] = dot(permt[...], hid[g]).astype(BF16).reshape(8, 16, QW)

    y_order = (4, 3, 5, 2, 6, 0)

    def reduce_send_y(block, ry, f, d):
        for e in (2, 1, 3):
            yy = ypeer(e)
            k = y_order.index(d)
            rcopy(block(yy), ry.at[d, e], s_all.at[5], r_y.at[k], (z * NY + yy, t)).start()

    def reduce_start(ry, rn, f):
        for d in (4, 3, 5, 2, 6):
            zz = zpeer(d)
            reduce_send_y(lambda yy: psend.at[zz * NY + yy], ry, f, d)
            if d == 4:
                for k, dd in enumerate((1, 7)):
                    near = zpeer(dd)
                    rcopy(
                        psend.at[pl.ds(near * NY, NY)], rn.at[pl.ds(NY * k, NY)], s_all.at[5], r_z.at[0],
                        (near * NY + y, t),
                    ).start()

    def reduce_finish(ry, rn, zs, rz, f, between=()):
        def with_y(total, d):
            wait_recv(ry.at[d, pl.ds(1, NY - 1)], r_y.at[y_order.index(d)])
            for e in range(1, NY):
                total = total + ry[d, e].astype(F32)
            return total

        for d in (4, 3, 5, 2, 6):
            zz = zpeer(d)
            zs[d] = with_y(psend[zz * NY + y].astype(F32), d).astype(BF16)
            rcopy(zs.at[d], rz.at[d], s_all.at[5], r_z.at[1], (zz * NY + y, t)).start()
            if d == 4:
                wait_recv(rn.at[pl.ds(0, 2 * NY)], r_z.at[0])
                near = psend[pl.ds(z * NY, NY)].astype(F32) + rn[0:NY].astype(F32) + rn[NY : 2 * NY].astype(F32)
                znear[...] = near.astype(BF16)
                reduce_send_y(lambda yy: znear.at[yy], ry, f, 0)
            for at, step in between:
                if at == d:
                    relay_weights(step)
        own = with_y(znear[y].astype(F32), 0)
        wait_recv(rz.at[pl.ds(0, 5)], r_z.at[1])
        for d in (2, 6, 3, 5, 4):
            own = own + rz[d].astype(F32)
        wait_send(psend.at[pl.ds(0, 31)], s_all.at[5])
        return own

    ag1[kv] = (res1 * piece_factor(res1) * gsplit[0:16]).astype(BF16)
    start_gather(ag1, 0)
    forward_gather(ag1, 0, ((0, 0), (0, 1), (4, 2)))
    for k in range(3):
        forward_weights(k)
    for k in range(3, 6):
        start_weights(k)
    finish_gather(ag1, 0)
    pltpu.make_async_copy(bytes_of(2, 3), bytes_of(2, 3), loc_sem.at[1]).wait()
    finish_weights(0)
    finish_weights(1)
    feed_forward(ag1, up1, down1, 0)
    reduce_start(ry1, rn1, 0)
    for copy in l_mix:
        copy.wait()
    for k in range(2):
        for j in range(SEQ // 2):
            scan_b[j, :, STATE * k : STATE * k + STATE] = scan_f[2 * j + k].astype(BF16)
    branch = reduce_finish(ry1, rn1, zs1, rz1, 0, ((4, 3), (4, 4), (5, 5)))
    first = (res1 + 0.5 * branch).astype(BF16).astype(F32)

    row, col = iota2((16, 16), 0), iota2((16, 16), 1)
    mixer_gain = jnp.concatenate(
        [dot((col == (row // 4) * 4 + j).astype(BF16), mgain_ref[...]) for j in range(4)], axis=1
    )
    send_f[...] = (first * piece_factor(first) * mixer_gain).astype(BF16)
    exchange_tp(lambda tt: send_f, recv_f.at[t], 1)
    recv_f[t] = send_f[...]
    def silu(v):
        return v * jax.nn.sigmoid(v)

    def old_taps(tap_ref, buf_ref):
        taps = tap_ref[...].astype(F32)
        total = buf_ref[0].astype(F32) * taps[0:1]
        for k in range(1, 3):
            total = total + buf_ref[k].astype(F32) * taps[k : k + 1]
        return total, taps[3:4]

    conv_i, conv_w, conv_r = old_taps(tapi_ref, bufi_ref), old_taps(tapw_ref, bufw_ref), old_taps(tapr_ref, bufr_ref)
    head_row = iota2((1, GROUP), 1) // HEAD_DIM

    def per_head(ref):
        values = ref[...]
        wide = jnp.broadcast_to(values[:, 0:1], (1, GROUP))
        for h in range(1, 4):
            wide = jnp.where(head_row == h, values[:, h : h + 1], wide)
        return wide

    bias_row, rate_row, skip_row = per_head(bias_ref), jnp.exp(per_head(rate_ref)), per_head(skip_ref)
    ggain_row = as_row(ggain_ref)
    wait_recv(recv_f.at[pl.ds(0, NT - 1)], r_t.at[1])
    for k in range(3, 6):
        forward_weights(k)
    rows = dot(perm[...], recv_f[...].reshape(128, QW)).astype(BF16)
    for q in range(4):
        xrow[:, QW * q : QW * q + QW] = rows[32 * q : 32 * q + 32]
    mixed_in = xrow[...]

    def project(w):
        return dot(mixed_in, w[...]).astype(BF16).astype(F32)

    wide, narrow = project(pgi), project(pwr)
    gate_z, input_new = wide[:, :GROUP], wide[:, GROUP:]
    write_new, read_new = narrow[:, :STATE], narrow[:, STATE:]
    step_raw4 = dot_nt(mixed_in, psv[...]).astype(BF16).astype(F32)
    xc = silu(conv_i[0] + input_new * conv_i[1])
    bc = silu(conv_w[0] + write_new * conv_w[1])
    rc = silu(conv_r[0] + read_new * conv_r[1])
    lane_head = iota2((SEQ, GROUP), 1) // HEAD_DIM
    step_raw = jnp.zeros((SEQ, GROUP), F32)
    for h in range(4):
        step_raw = jnp.where(lane_head == h, step_raw4[:, h : h + 1], step_raw)
    pre = step_raw + bias_row
    step = jnp.maximum(pre, 0.0) + jnp.log1p(jnp.exp(-jnp.abs(pre)))
    retain = jnp.exp(-step * rate_row)
    u = step * xc
    rc_pair = jnp.concatenate([rc, rc], axis=1)
    sub, half = iota2((8, 2 * STATE), 0), iota2((8, 2 * STATE), 1) // STATE
    reads = []
    for g in range(4):
        acc = jnp.zeros((8, GROUP), F32)
        for j in range(4):
            row = jnp.where(sub == 2 * j + half, rc_pair[8 * g : 8 * g + 8], 0.0).astype(BF16)
            acc = acc + dot_nt(row, scan_b[4 * g + j])
        reads.append(acc)
    read = jnp.concatenate(reads, axis=0)
    head = retain * read + u * jnp.sum(bc * rc, axis=1, keepdims=True) + skip_row * xc
    gated = head.astype(BF16).astype(F32) * silu(gate_z)
    gated = gated * lax.rsqrt(jnp.mean(gated * gated, axis=1, keepdims=True) + EPS) * ggain_row
    part = dot(gated.astype(BF16), pov[...]).astype(BF16)
    stacked = jnp.concatenate([part[:, QW * q : QW * q + QW] for q in range(4)], axis=0)
    send_o[...] = dot(permt[...], stacked).astype(BF16).reshape(NT, 16, QW)
    exchange_tp(lambda tt: send_o.at[tt], recv_o.at[t], 2)
    recv_o[t] = send_o[t]
    pltpu.make_async_copy(bytes_of(5, 3), bytes_of(5, 3), loc_sem.at[2]).wait()
    u_cols = jnp.transpose(u)
    for b in range(SEQ):
        for h in range(4):
            rows_h = slice(HEAD_DIM * h, HEAD_DIM * h + HEAD_DIM)
            keep = jnp.broadcast_to(retain[b : b + 1, HEAD_DIM * h : HEAD_DIM * h + 1], (HEAD_DIM, STATE))
            scan_f[b, rows_h, :] = keep * scan_f[b, rows_h, :] + u_cols[rows_h, b : b + 1] * bc[b : b + 1]
    l_state = local(scan_f, state_ref, 0)
    wait_recv(recv_o.at[pl.ds(0, NT - 1)], r_t.at[2])
    mixed = first
    for k in range(NT):
        mixed = mixed + recv_o[k].astype(F32)
    res2 = mixed.astype(BF16).astype(F32)

    ag2[kv] = (res2 * piece_factor(res2) * gsplit[16:32]).astype(BF16)
    start_gather(ag2, 1)
    forward_gather(ag2, 1)
    finish_gather(ag2, 1)
    finish_weights(3)
    finish_weights(4)
    feed_forward(ag2, up2, down2, 3)
    reduce_start(ry2, rn2, 1)
    branch = reduce_finish(ry2, rn2, zs2, rz2, 1)
    final = (res2 + 0.5 * branch).astype(BF16)

    row, col = iota2((64, 16), 0), iota2((64, 16), 1)
    spread = ((col == (row // 16) * 4 + row % 16) & (row % 16 < 4)).astype(BF16)
    for h in range(2):
        block = dot(spread, final[:, 256 * h : 256 * h + 256]).astype(BF16).reshape(4, 16, 256)
        for q in range(4):
            send_q[2 * q + h] = block[q]
    exchange_tp(lambda tt: send_q.at[tt], recv_q.at[t], 3)
    recv_q[t] = send_q[t]
    row, col = iota2((32, 128), 0), iota2((32, 128), 1)
    pick32 = (col == (row // 4) * 16 + row % 4).astype(BF16)
    wait_recv(recv_q.at[pl.ds(0, NT - 1)], r_t.at[3])
    out_ref[...] = dot(pick32, recv_q[...].reshape(128, 256)).astype(BF16)

    l_state.wait()
    for k, block in enumerate((recv_r, recv_f, recv_o, recv_q)):
        wait_send(block.at[pl.ds(0, NT - 1)], s_all.at[k])


def per_device(
    residual, first_gain, first_gate, first_lift, first_down, mixer_gain,
    proj_gate, proj_input, proj_write, proj_read, proj_step,
    step_bias, rate_log, skip_gain, taps_input, taps_write, taps_read,
    buffer_input, buffer_write, buffer_read, scan_state, group_gain, proj_output,
    second_gain, second_gate, second_lift, second_down,
):
    scan = scan_state.reshape(SEQ, GROUP, STATE)
    anym = pl.BlockSpec(memory_space=pl.ANY)
    hid_cols = first_gate.shape[1]
    dma = pltpu.SemaphoreType.DMA
    small = (
        residual, first_gain.reshape(2, 128), second_gain.reshape(2, 128), mixer_gain.reshape(16, 128),
        group_gain.reshape(2, 128), step_bias.reshape(1, 4), rate_log.reshape(1, 4), skip_gain.reshape(1, 4),
        taps_input, taps_write, taps_read,
        buffer_input.transpose(1, 0, 2), buffer_write.transpose(1, 0, 2), buffer_read.transpose(1, 0, 2),
    )
    out, state = pl.pallas_call(
        kernel,
        out_shape=(
            pltpu.VMEM((SEQ, GROUP), BF16),
            pltpu.VMEM((SEQ, GROUP, STATE), F32),
        ),
        in_specs=[anym] * 27,
        out_specs=(pl.BlockSpec(memory_space=pltpu.VMEM), anym),
        scratch_shapes=[
            *[pltpu.VMEM(a.shape, a.dtype) for a in small],
            pltpu.VMEM((NT, 16, GROUP), BF16),
            pltpu.VMEM((NT, 16, GROUP), BF16),
            *[pltpu.VMEM((2 * hid_cols, D), BF16), pltpu.VMEM((hid_cols, D), BF16)] * 2,
            pltpu.VMEM((NKV, 16, QW), BF16),
            pltpu.VMEM((NKV, 16, QW), BF16),
            pltpu.VMEM((128, 128), BF16),
            pltpu.VMEM((128, 128), BF16),
            pltpu.VMEM((128, D), BF16),
            pltpu.VMEM((4, 128, QW), BF16),
            pltpu.VMEM((NKV, 16, QW), BF16),
            pltpu.VMEM((NY, 16, QW), BF16),
            *[pltpu.VMEM((NZ, NY, 16, QW), BF16), pltpu.VMEM((2 * NY, 16, QW), BF16), pltpu.VMEM((NZ, 16, QW), BF16), pltpu.VMEM((NZ, 16, QW), BF16)] * 2,
            pltpu.VMEM((16, QW), BF16),
            pltpu.VMEM((NT, 16, QW), BF16),
            pltpu.VMEM((NT, 16, QW), BF16),
            pltpu.VMEM((NT, 16, QW), BF16),
            pltpu.VMEM((NT, 16, GROUP), BF16),
            pltpu.VMEM((NT, 16, GROUP), BF16),
            pltpu.VMEM((D, 512), BF16),
            pltpu.VMEM((D, 256), BF16),
            pltpu.VMEM((4, D), BF16),
            pltpu.VMEM((256, D), BF16),
            pltpu.VMEM((SEQ, GROUP, STATE), F32),
            pltpu.VMEM((SEQ // 2, GROUP, 2 * STATE), BF16),
            pltpu.VMEM((SEQ, D), BF16),
            pltpu.VMEM((32, QW), F32),
            dma((10,)), dma((6,)), dma((4,)),
            dma((6,)), dma((6,)), dma((6,)), dma((6,)),
            dma((9,)), dma((6,)), dma((2,)), dma((14,)), pltpu.SemaphoreType.REGULAR((2,)),
        ],
        compiler_params=pltpu.CompilerParams(
            collective_id=0, has_side_effects=True, vmem_limit_bytes=56 * 1024 * 1024
        ),
        name="layer",
    )(
        *small,
        first_gate.T, first_lift.T, first_down, second_gate.T, second_lift.T, second_down,
        proj_gate, proj_input, proj_write, proj_read, proj_step.T, proj_output, scan,
    )
    return out, state.reshape(scan_state.shape)


def solution(mesh):
    placed = (
        P("kv", "tp"), P("tp"), P("tp", "kv"), P("tp", "kv"), P("kv", "tp"), P(),
        P(None, "tp"), P(None, "tp"), P(None, "tp"), P(None, "tp"), P(None, "tp"),
        P("tp"), P("tp"), P("tp"), P(None, "tp"), P(None, "tp"), P(None, "tp"),
        P("kv", None, "tp"), P("kv", None, "tp"), P("kv", None, "tp"), P("kv", "tp", None, None),
        P("tp"), P("tp", None), P("tp"), P("tp", "kv"), P("tp", "kv"), P("kv", "tp"),
    )
    return jax.shard_map(
        per_device,
        mesh=mesh,
        in_specs=placed,
        out_specs=(P("kv", "tp"), P("kv", "tp", None, None)),
        check_vma=False,
    )
```

```python
import jax
import jax.numpy as jnp
from jax import lax
from jax.experimental import pallas as pl
from jax.experimental.pallas import tpu as pltpu
from jax.sharding import PartitionSpec as P

D = 2048
HEAD_DIM = 64
STATE = 128
EPS = 1e-06

NZ, NY, NT = 8, 4, 8
NKV = NZ * NY
RPT = 4
QW = 512
SEQ = 32
GROUP = 256
MESH = pl.DeviceIdType.MESH
F32, BF16 = jnp.float32, jnp.bfloat16


def dot(a, b):
    return jnp.dot(a, b, preferred_element_type=F32)


def dot_nt(a, b):
    return lax.dot_general(a, b, (((1,), (1,)), ((), ())), preferred_element_type=F32)


def iota2(shape, dim):
    return lax.broadcasted_iota(jnp.int32, shape, dim)


def gather_rows(n):
    shape = (16 * n, 16 * n)
    row, col = iota2(shape, 0), iota2(shape, 1)
    q, rest = row // (4 * n), row % (4 * n)
    return (col == (rest // 4) * 16 + q * 4 + rest % 4).astype(BF16)


def scatter_rows(n):
    shape = (16 * n, 16 * n)
    row, col = iota2(shape, 0), iota2(shape, 1)
    q, rest = col // (4 * n), col % (4 * n)
    return (row == (rest // 4) * 16 + q * 4 + rest % 4).astype(BF16)


def piece_factor(piece):
    square = piece * piece
    total = square[:, 0:128] + square[:, 128:256] + square[:, 256:384] + square[:, 384:512]
    total = total + pltpu.roll(total, 8, 0)
    total = total + pltpu.roll(total, 4, 0)
    return lax.rsqrt(jnp.sum(total, axis=1, keepdims=True) / D + EPS)


def kernel(*refs):
    small_in, refs = refs[:14], refs[14:]
    (fg_ref, fl_ref, fd_ref, sg_ref, sl_ref, sd_ref), refs = refs[:6], refs[6:]
    (pg_ref, pi_ref, pw_ref, pr_ref, ps_ref, po_ref, scan_ref), refs = refs[:7], refs[7:]
    (out_ref, state_ref), refs = refs[:2], refs[2:]
    small, refs = refs[:14], refs[14:]
    res_ref, gain1_ref, gain2_ref, mgain_ref, ggain_ref, bias_ref, rate_ref, skip_ref = small[:8]
    tapi_ref, tapw_ref, tapr_ref, bufi_ref, bufw_ref, bufr_ref = small[8:]
    (
        msg, recv_r, up1, down1, up2, down2,
        ag1, ag2, perm, permt, lhs_v, hid, psend, znear, ry1, rn1, zs1, rz1, ry2, rn2, zs2, rz2,
        send_f, recv_f, recv_o, send_o, send_q, recv_q,
        pgi, pwr, psv, pov, scan_f, scan_b, xrow, gsplit,
        loc_sem, s_all, r_t, s_w, r_wx, r_wo, r_wc, r_ag, r_y, r_z, in_sem, ready,
    ) = refs
    kv = lax.axis_index("kv")
    t = lax.axis_index("tp")
    z, y = kv // NY, kv % NY
    core = t % 2

    def zpeer(d):
        return lax.rem(z + d, NZ)

    def ypeer(d):
        return lax.rem(y + d, NY)

    def tpeer(d):
        return lax.rem(t + d, NT)

    def rcopy(src, dst, ssem, rsem, dev):
        return pltpu.make_async_remote_copy(
            src_ref=src, dst_ref=dst, send_sem=ssem, recv_sem=rsem, device_id=dev, device_id_type=MESH
        )

    def wait_recv(block, rsem):
        rcopy(block, block, s_all.at[0], rsem, (kv, tpeer(1))).wait_recv()

    def wait_send(block, ssem):
        rcopy(block, block, ssem, r_t.at[0], (kv, tpeer(1))).wait_send()

    def local(src, dst, k):
        copy = pltpu.make_async_copy(src, dst, loc_sem.at[k])
        copy.start()
        return copy

    barrier = pltpu.get_barrier_semaphore()
    peers = [(kv, tpeer(d)) for d in range(1, NT)]
    peers += [(zpeer(d) * NY + y, t) for d in (1, 7)]
    peers += [(z * NY + ypeer(d), t) for d in range(1, NY)]
    for dev in peers:
        pl.semaphore_signal(barrier, inc=1, device_id=dev, device_id_type=MESH)
    l_small = []
    for k in range(14):
        copy = pltpu.make_async_copy(small_in[k], small[k], in_sem.at[k])
        copy.start()
        l_small.append(copy)
    hid_units = fg_ref.shape[0]
    sources = (fg_ref, fl_ref, fd_ref, sg_ref, sl_ref, sd_ref)
    gathered = ((up1, 0), (up1, hid_units), (down1, 0), (up2, 0), (up2, hid_units), (down2, 0))

    def block_of(k, s, first=0, rows=None):
        dst, top = gathered[k]
        return dst.at[pl.ds(top + first, rows or hid_units), pl.ds(pl.multiple_of(s * 256, 256), 256)]

    def bytes_of(k, count):
        dst = gathered[k][0]
        return dst.at[:, pl.ds(0, 256 * count)]

    for k in range(3):
        local(sources[k], block_of(k, t), 1)
    for k in range(3):
        l_small[k].wait()

    def as_row(ref):
        wide = ref[...].astype(F32)
        return jnp.concatenate([wide[k : k + 1] for k in range(wide.shape[0])], axis=1)

    row, col = iota2((128, 32), 0), iota2((128, 32), 1)
    give = ((col == (row // 16) * 4 + row % 16) & (row % 16 < 4)).astype(BF16)
    kind = (iota2((128, GROUP), 0) % 16) // 4
    body = dot(give, res_ref[...])
    body = jnp.where(kind == 1, as_row(gain1_ref), jnp.where(kind == 2, as_row(gain2_ref), body))
    msg[...] = body.astype(BF16).reshape(NT, 16, GROUP)
    recv_r[t] = msg[t]

    pl.semaphore_wait(barrier, len(peers))

    def exchange_tp(block, dst, k):
        base = t - core
        far, right, left = lax.rem(base + 4, NT), lax.rem(base + 2, NT), lax.rem(base + 6, NT)
        for tt in (far, far + 1, right, left, right + 1, left + 1, base + 1 - core):
            rcopy(block(tt), dst, s_all.at[k], r_t.at[k], (kv, tt)).start()

    exchange_tp(lambda tt: msg.at[tt], recv_r.at[t], 0)
    for d in (1, 7):
        pl.semaphore_signal(ready.at[0], inc=1, device_id=(zpeer(d) * NY + y, t), device_id_type=MESH)

    partner = t + 1 - 2 * core
    left, right, across = lax.rem(t + NT - 2, NT), lax.rem(t + 2, NT), lax.rem(t + 4, NT)
    cuts = (hid_units, 0, 96)

    def sem_of(k):
        return 2 * (k // 3) + (k % 3) // 2

    def start_weights(k):
        for tt in (right, left):
            rcopy(sources[k], block_of(k, t), s_w.at[sem_of(k)], r_wx.at[sem_of(k)], (kv, tt)).start()
        rcopy(sources[k], block_of(k, t), s_w.at[sem_of(k)], r_wc.at[sem_of(k)], (kv, partner)).start()

    def relay_weights(k):
        if k % 3 != 1:
            wait_recv(bytes_of(k, 2), r_wx.at[sem_of(k)])
        cut = cuts[k % 3]
        if cut > 0:
            part = block_of(k, left, 0, cut)
            rcopy(part, part, s_w.at[sem_of(k)], r_wo.at[sem_of(k)], (kv, right)).start()
        if cut < hid_units:
            part = block_of(k, right, cut, hid_units - cut)
            rcopy(part, part, s_w.at[sem_of(k)], r_wo.at[sem_of(k)], (kv, left)).start()
        for ss in (left, right):
            rcopy(block_of(k, ss), block_of(k, ss), s_w.at[sem_of(k)], r_wc.at[sem_of(k)], (kv, partner)).start()

    def forward_weights(k):
        if k % 3 != 1:
            wait_recv(bytes_of(k, 1), r_wo.at[sem_of(k)])
        rcopy(block_of(k, across), block_of(k, across), s_w.at[sem_of(k)], r_wc.at[sem_of(k)], (kv, partner)).start()

    def finish_weights(k):
        if k % 3 != 1:
            wait_recv(bytes_of(k, 4), r_wc.at[sem_of(k)])

    def sent_weights(k):
        wait_send(bytes_of(k, 7), s_w.at[sem_of(k)])

    for k in range(3):
        start_weights(k)

    l_mix = [
        local(pg_ref, pgi.at[:, pl.ds(0, 256)], 3), local(pi_ref, pgi.at[:, pl.ds(256, 256)], 4),
        local(pw_ref, pwr.at[:, pl.ds(0, 128)], 5), local(pr_ref, pwr.at[:, pl.ds(128, 128)], 6),
        local(ps_ref, psv, 7), local(po_ref, pov, 8), local(scan_ref, scan_f, 9),
    ]
    for k in range(3, 6):
        local(sources[k], block_of(k, t), 2)

    pl.semaphore_wait(ready.at[0], 2)
    for d in (2, 6):
        pl.semaphore_signal(ready.at[1], inc=1, device_id=(zpeer(d) * NY + y, t), device_id_type=MESH)
    perm[...] = gather_rows(NT)
    permt[...] = scatter_rows(NT)
    for k in range(3, 14):
        l_small[k].wait()
    wait_recv(recv_r.at[pl.ds(0, NT - 1)], r_t.at[0])

    pl.semaphore_wait(ready.at[1], 2)
    row, col = iota2((48, 64), 0), iota2((48, 64), 1)
    pick = (col == ((row % 16) // 4) * 16 + (row // 16) * 4 + row % 4).astype(BF16)
    halves = []
    for h in range(2):
        block = jnp.concatenate([recv_r[2 * q + h] for q in range(4)], axis=0)
        halves.append(dot(pick, block))
    both = jnp.concatenate(halves, axis=1)
    res1 = both[0:16]
    gsplit[...] = both[16:48]

    ag_order = ((2, 0), (6, 0), (3, 0), (5, 0), (0, 1), (0, 3), (4, 0), (0, 2))

    def gather_send(ag, slot, f, d, e, dev):
        k = ag_order.index((d, e)) if (d, e) in ag_order else 8
        rcopy(ag.at[slot], ag.at[slot], s_all.at[4], r_ag.at[k], (dev, t)).start()

    def start_gather(ag, f):
        for d in (4, 3, 5, 2, 6, 1, 7):
            gather_send(ag, kv, f, d, 0, zpeer(d) * NY + y)
        for e in (2, 1, 3):
            gather_send(ag, kv, f, 0, e, z * NY + ypeer(e))

    def forward_gather(ag, f, between=()):
        for k, (d, e) in enumerate(ag_order):
            for at, step in between:
                if at == k:
                    relay_weights(step)
            slot = lax.rem(z - d + NZ, NZ) * NY + lax.rem(y - e + NY, NY)
            wait_recv(ag.at[slot], r_ag.at[k])
            if e == 0:
                for ee in (2, 1, 3):
                    gather_send(ag, slot, f, d, ee, z * NY + ypeer(ee))
            else:
                for dd in (1, 7):
                    gather_send(ag, slot, f, dd, e, zpeer(dd) * NY + y)

    def finish_gather(ag, f):
        wait_recv(ag.at[pl.ds(0, 23)], r_ag.at[8])

    def feed_forward(ag, up, down, k):
        for g in range(NKV // 8):
            rows = dot(perm[...], ag[8 * g : 8 * g + 8].reshape(128, QW)).astype(BF16)
            for q in range(4):
                lhs_v[32 * g : 32 * g + 32, QW * q : QW * q + QW] = rows[32 * q : 32 * q + 32]
        lhs = lhs_v[...]
        gate, lift = dot_nt(lhs, up[0:hid_units]), dot_nt(lhs, up[hid_units : 2 * hid_units])
        finish_weights(k + 2)
        hidden = (gate * jax.nn.sigmoid(gate) * lift).astype(BF16)
        out = dot(hidden, down[...]).astype(BF16)
        for g in range(NKV // 8):
            for q in range(4):
                hid[g, 32 * q : 32 * q + 32] = out[32 * g : 32 * g + 32, QW * q : QW * q + QW]
        for g in range(NKV // 8):
            psend[8 * g : 8 * g + 8] = dot(permt[...], hid[g]).astype(BF16).reshape(8, 16, QW)

    y_order = (4, 3, 5, 2, 6, 0)

    def reduce_send_y(block, ry, f, d):
        for e in (2, 1, 3):
            yy = ypeer(e)
            k = y_order.index(d)
            rcopy(block(yy), ry.at[d, e], s_all.at[5], r_y.at[k], (z * NY + yy, t)).start()

    def reduce_start(ry, rn, f):
        for d in (4, 3, 5, 2, 6):
            zz = zpeer(d)
            reduce_send_y(lambda yy: psend.at[zz * NY + yy], ry, f, d)
            if d == 4:
                for k, dd in enumerate((1, 7)):
                    near = zpeer(dd)
                    rcopy(
                        psend.at[pl.ds(near * NY, NY)], rn.at[pl.ds(NY * k, NY)], s_all.at[5], r_z.at[0],
                        (near * NY + y, t),
                    ).start()

    def reduce_finish(ry, rn, zs, rz, f, between=()):
        def with_y(total, d):
            wait_recv(ry.at[d, pl.ds(1, NY - 1)], r_y.at[y_order.index(d)])
            for e in range(1, NY):
                total = total + ry[d, e].astype(F32)
            return total

        for d in (4, 3, 5, 2, 6):
            zz = zpeer(d)
            zs[d] = with_y(psend[zz * NY + y].astype(F32), d).astype(BF16)
            rcopy(zs.at[d], rz.at[d], s_all.at[5], r_z.at[1], (zz * NY + y, t)).start()
            if d == 4:
                wait_recv(rn.at[pl.ds(0, 2 * NY)], r_z.at[0])
                near = psend[pl.ds(z * NY, NY)].astype(F32) + rn[0:NY].astype(F32) + rn[NY : 2 * NY].astype(F32)
                znear[...] = near.astype(BF16)
                reduce_send_y(lambda yy: znear.at[yy], ry, f, 0)
            for at, step in between:
                if at == d:
                    relay_weights(step)
        own = with_y(znear[y].astype(F32), 0)
        wait_recv(rz.at[pl.ds(0, 5)], r_z.at[1])
        for d in (2, 6, 3, 5, 4):
            own = own + rz[d].astype(F32)
        return own

    ag1[kv] = (res1 * piece_factor(res1) * gsplit[0:16]).astype(BF16)
    start_gather(ag1, 0)
    forward_gather(ag1, 0, ((0, 0), (0, 1), (4, 2)))
    for k in range(3):
        forward_weights(k)
    for k in range(3, 6):
        start_weights(k)
    finish_gather(ag1, 0)
    pltpu.make_async_copy(bytes_of(2, 3), bytes_of(2, 3), loc_sem.at[1]).wait()
    finish_weights(0)
    finish_weights(1)
    feed_forward(ag1, up1, down1, 0)
    reduce_start(ry1, rn1, 0)
    wait_send(ag1.at[pl.ds(0, 31)], s_all.at[4])
    sent_weights(0)
    sent_weights(2)
    for copy in l_mix:
        copy.wait()
    for k in range(2):
        for j in range(SEQ // 2):
            scan_b[j, :, STATE * k : STATE * k + STATE] = scan_f[2 * j + k].astype(BF16)
    branch = reduce_finish(ry1, rn1, zs1, rz1, 0, ((4, 3), (4, 4), (5, 5)))
    first = (res1 + 0.5 * branch).astype(BF16).astype(F32)

    row, col = iota2((16, 16), 0), iota2((16, 16), 1)
    mixer_gain = jnp.concatenate(
        [dot((col == (row // 4) * 4 + j).astype(BF16), mgain_ref[...]) for j in range(4)], axis=1
    )
    send_f[...] = (first * piece_factor(first) * mixer_gain).astype(BF16)
    exchange_tp(lambda tt: send_f, recv_f.at[t], 1)
    recv_f[t] = send_f[...]
    wait_send(psend.at[pl.ds(0, 31)], s_all.at[5])
    def silu(v):
        return v * jax.nn.sigmoid(v)

    def old_taps(tap_ref, buf_ref):
        taps = tap_ref[...].astype(F32)
        total = buf_ref[0].astype(F32) * taps[0:1]
        for k in range(1, 3):
            total = total + buf_ref[k].astype(F32) * taps[k : k + 1]
        return total, taps[3:4]

    conv_i, conv_w, conv_r = old_taps(tapi_ref, bufi_ref), old_taps(tapw_ref, bufw_ref), old_taps(tapr_ref, bufr_ref)
    head_row = iota2((1, GROUP), 1) // HEAD_DIM

    def per_head(ref):
        values = ref[...]
        wide = jnp.broadcast_to(values[:, 0:1], (1, GROUP))
        for h in range(1, 4):
            wide = jnp.where(head_row == h, values[:, h : h + 1], wide)
        return wide

    bias_row, rate_row, skip_row = per_head(bias_ref), jnp.exp(per_head(rate_ref)), per_head(skip_ref)
    ggain_row = as_row(ggain_ref)
    wait_recv(recv_f.at[pl.ds(0, NT - 1)], r_t.at[1])
    rows = dot(perm[...], recv_f[...].reshape(128, QW)).astype(BF16)
    for q in range(4):
        xrow[:, QW * q : QW * q + QW] = rows[32 * q : 32 * q + 32]
    mixed_in = xrow[...]

    def project(w):
        return dot(mixed_in, w[...]).astype(BF16).astype(F32)

    wide, narrow = project(pgi), project(pwr)
    gate_z, input_new = wide[:, :GROUP], wide[:, GROUP:]
    write_new, read_new = narrow[:, :STATE], narrow[:, STATE:]
    step_raw4 = dot_nt(mixed_in, psv[...]).astype(BF16).astype(F32)
    xc = silu(conv_i[0] + input_new * conv_i[1])
    bc = silu(conv_w[0] + write_new * conv_w[1])
    rc = silu(conv_r[0] + read_new * conv_r[1])
    lane_head = iota2((SEQ, GROUP), 1) // HEAD_DIM
    step_raw = jnp.zeros((SEQ, GROUP), F32)
    for h in range(4):
        step_raw = jnp.where(lane_head == h, step_raw4[:, h : h + 1], step_raw)
    pre = step_raw + bias_row
    step = jnp.maximum(pre, 0.0) + jnp.log1p(jnp.exp(-jnp.abs(pre)))
    retain = jnp.exp(-step * rate_row)
    u = step * xc
    rc_pair = jnp.concatenate([rc, rc], axis=1)
    sub, half = iota2((8, 2 * STATE), 0), iota2((8, 2 * STATE), 1) // STATE
    reads = []
    for g in range(4):
        acc = jnp.zeros((8, GROUP), F32)
        for j in range(4):
            row = jnp.where(sub == 2 * j + half, rc_pair[8 * g : 8 * g + 8], 0.0).astype(BF16)
            acc = acc + dot_nt(row, scan_b[4 * g + j])
        reads.append(acc)
    read = jnp.concatenate(reads, axis=0)
    head = retain * read + u * jnp.sum(bc * rc, axis=1, keepdims=True) + skip_row * xc
    gated = head.astype(BF16).astype(F32) * silu(gate_z)
    gated = gated * lax.rsqrt(jnp.mean(gated * gated, axis=1, keepdims=True) + EPS) * ggain_row
    part = dot(gated.astype(BF16), pov[...]).astype(BF16)
    stacked = jnp.concatenate([part[:, QW * q : QW * q + QW] for q in range(4)], axis=0)
    send_o[...] = dot(permt[...], stacked).astype(BF16).reshape(NT, 16, QW)
    exchange_tp(lambda tt: send_o.at[tt], recv_o.at[t], 2)
    recv_o[t] = send_o[t]
    for k in range(3, 6):
        forward_weights(k)
    pltpu.make_async_copy(bytes_of(5, 3), bytes_of(5, 3), loc_sem.at[2]).wait()
    u_cols = jnp.transpose(u)
    for b in range(SEQ):
        for h in range(4):
            rows_h = slice(HEAD_DIM * h, HEAD_DIM * h + HEAD_DIM)
            keep = jnp.broadcast_to(retain[b : b + 1, HEAD_DIM * h : HEAD_DIM * h + 1], (HEAD_DIM, STATE))
            scan_f[b, rows_h, :] = keep * scan_f[b, rows_h, :] + u_cols[rows_h, b : b + 1] * bc[b : b + 1]
    l_state = local(scan_f, state_ref, 0)
    wait_recv(recv_o.at[pl.ds(0, NT - 1)], r_t.at[2])
    mixed = first
    for k in range(NT):
        mixed = mixed + recv_o[k].astype(F32)
    res2 = mixed.astype(BF16).astype(F32)

    ag2[kv] = (res2 * piece_factor(res2) * gsplit[16:32]).astype(BF16)
    start_gather(ag2, 1)
    forward_gather(ag2, 1)
    finish_gather(ag2, 1)
    finish_weights(3)
    finish_weights(4)
    feed_forward(ag2, up2, down2, 3)
    reduce_start(ry2, rn2, 1)
    branch = reduce_finish(ry2, rn2, zs2, rz2, 1)
    final = (res2 + 0.5 * branch).astype(BF16)

    row, col = iota2((64, 16), 0), iota2((64, 16), 1)
    spread = ((col == (row // 16) * 4 + row % 16) & (row % 16 < 4)).astype(BF16)
    for h in range(2):
        block = dot(spread, final[:, 256 * h : 256 * h + 256]).astype(BF16).reshape(4, 16, 256)
        for q in range(4):
            send_q[2 * q + h] = block[q]
    exchange_tp(lambda tt: send_q.at[tt], recv_q.at[t], 3)
    recv_q[t] = send_q[t]
    row, col = iota2((32, 128), 0), iota2((32, 128), 1)
    pick32 = (col == (row // 4) * 16 + row % 4).astype(BF16)
    wait_recv(recv_q.at[pl.ds(0, NT - 1)], r_t.at[3])
    out_ref[...] = dot(pick32, recv_q[...].reshape(128, 256)).astype(BF16)

    wait_send(ag2.at[pl.ds(0, 31)], s_all.at[4])
    wait_send(psend.at[pl.ds(0, 31)], s_all.at[5])
    sent_weights(3)
    sent_weights(5)
    l_state.wait()
    for k, block in enumerate((recv_r, recv_f, recv_o, recv_q)):
        wait_send(block.at[pl.ds(0, NT - 1)], s_all.at[k])


def per_device(
    residual, first_gain, first_gate, first_lift, first_down, mixer_gain,
    proj_gate, proj_input, proj_write, proj_read, proj_step,
    step_bias, rate_log, skip_gain, taps_input, taps_write, taps_read,
    buffer_input, buffer_write, buffer_read, scan_state, group_gain, proj_output,
    second_gain, second_gate, second_lift, second_down,
):
    scan = scan_state.reshape(SEQ, GROUP, STATE)
    anym = pl.BlockSpec(memory_space=pl.ANY)
    hid_cols = first_gate.shape[1]
    dma = pltpu.SemaphoreType.DMA
    small = (
        residual, first_gain.reshape(2, 128), second_gain.reshape(2, 128), mixer_gain.reshape(16, 128),
        group_gain.reshape(2, 128), step_bias.reshape(1, 4), rate_log.reshape(1, 4), skip_gain.reshape(1, 4),
        taps_input, taps_write, taps_read,
        buffer_input.transpose(1, 0, 2), buffer_write.transpose(1, 0, 2), buffer_read.transpose(1, 0, 2),
    )
    out, state = pl.pallas_call(
        kernel,
        out_shape=(
            pltpu.VMEM((SEQ, GROUP), BF16),
            pltpu.VMEM((SEQ, GROUP, STATE), F32),
        ),
        in_specs=[anym] * 27,
        out_specs=(pl.BlockSpec(memory_space=pltpu.VMEM), anym),
        scratch_shapes=[
            *[pltpu.VMEM(a.shape, a.dtype) for a in small],
            pltpu.VMEM((NT, 16, GROUP), BF16),
            pltpu.VMEM((NT, 16, GROUP), BF16),
            *[pltpu.VMEM((2 * hid_cols, D), BF16), pltpu.VMEM((hid_cols, D), BF16)] * 2,
            pltpu.VMEM((NKV, 16, QW), BF16),
            pltpu.VMEM((NKV, 16, QW), BF16),
            pltpu.VMEM((128, 128), BF16),
            pltpu.VMEM((128, 128), BF16),
            pltpu.VMEM((128, D), BF16),
            pltpu.VMEM((4, 128, QW), BF16),
            pltpu.VMEM((NKV, 16, QW), BF16),
            pltpu.VMEM((NY, 16, QW), BF16),
            *[pltpu.VMEM((NZ, NY, 16, QW), BF16), pltpu.VMEM((2 * NY, 16, QW), BF16), pltpu.VMEM((NZ, 16, QW), BF16), pltpu.VMEM((NZ, 16, QW), BF16)] * 2,
            pltpu.VMEM((16, QW), BF16),
            pltpu.VMEM((NT, 16, QW), BF16),
            pltpu.VMEM((NT, 16, QW), BF16),
            pltpu.VMEM((NT, 16, QW), BF16),
            pltpu.VMEM((NT, 16, GROUP), BF16),
            pltpu.VMEM((NT, 16, GROUP), BF16),
            pltpu.VMEM((D, 512), BF16),
            pltpu.VMEM((D, 256), BF16),
            pltpu.VMEM((4, D), BF16),
            pltpu.VMEM((256, D), BF16),
            pltpu.VMEM((SEQ, GROUP, STATE), F32),
            pltpu.VMEM((SEQ // 2, GROUP, 2 * STATE), BF16),
            pltpu.VMEM((SEQ, D), BF16),
            pltpu.VMEM((32, QW), F32),
            dma((10,)), dma((6,)), dma((4,)),
            dma((4,)), dma((4,)), dma((4,)), dma((4,)),
            dma((9,)), dma((6,)), dma((2,)), dma((14,)), pltpu.SemaphoreType.REGULAR((2,)),
        ],
        compiler_params=pltpu.CompilerParams(
            collective_id=0, has_side_effects=True, vmem_limit_bytes=56 * 1024 * 1024
        ),
        name="layer",
    )(
        *small,
        first_gate.T, first_lift.T, first_down, second_gate.T, second_lift.T, second_down,
        proj_gate, proj_input, proj_write, proj_read, proj_step.T, proj_output, scan,
    )
    return out, state.reshape(scan_state.shape)


def solution(mesh):
    placed = (
        P("kv", "tp"), P("tp"), P("tp", "kv"), P("tp", "kv"), P("kv", "tp"), P(),
        P(None, "tp"), P(None, "tp"), P(None, "tp"), P(None, "tp"), P(None, "tp"),
        P("tp"), P("tp"), P("tp"), P(None, "tp"), P(None, "tp"), P(None, "tp"),
        P("kv", None, "tp"), P("kv", None, "tp"), P("kv", None, "tp"), P("kv", "tp", None, None),
        P("tp"), P("tp", None), P("tp"), P("tp", "kv"), P("tp", "kv"), P("kv", "tp"),
    )
    return jax.shard_map(
        per_device,
        mesh=mesh,
        in_specs=placed,
        out_specs=(P("kv", "tp"), P("kv", "tp", None, None)),
        check_vma=False,
    )
```
